32 devices in a mesh: sp: 8 (over z, y), tp: 4 (over x, core).
Axes of the slice: x: 2, y: 2, z: 4, core: 2. Of those that a mesh axis runs over, the one named last changes fastest.
Arguments:
- out_grad: bfloat16 [1536, 2048], P('sp'), may hold values from -6 to 6
- routes: int32 [1536, 2], P('sp'), may hold values from 0 to 7, all different within a row; in each aligned block of 192 rows (0 to 191, 192 to 383, ...) at most 96 rows name the same one
- route_weight: float32 [1536, 2], P('sp'), may hold values from 0.3 to 1.5
- expert_rows: bfloat16 [8, 8, 96, 2048], P(None, 'sp'), may hold values from -6 to 6
- gate_weight: bfloat16 [8, 2048, 1024], P('sp', None, 'tp'), may hold values from -0.125 to 0.125
- up_weight: bfloat16 [8, 2048, 1024], P('sp', None, 'tp'), may hold values from -0.125 to 0.125
- down_weight: bfloat16 [8, 1024, 2048], P('sp', 'tp'), may hold values from -0.1875 to 0.1875
- conv_input: bfloat16 [1536, 1024], P('sp', 'tp'), may hold values from -6 to 6
- out_gate: bfloat16 [1536, 1024], P('sp', 'tp'), may hold values from -6 to 6
- in_gate: bfloat16 [1536, 1024], P('sp', 'tp'), may hold values from -6 to 6
- taps: float32 [3, 1024], P(None, 'tp'), may hold values from -3 to 3
- out_weight: bfloat16 [2048, 1024], P(None, 'tp'), may hold values from -0.1875 to 0.1875
Outputs:
- gate_grad: bfloat16 [8, 2048, 1024], P('sp', None, 'tp')
- up_grad: bfloat16 [8, 2048, 1024], P('sp', None, 'tp')
- down_grad: bfloat16 [8, 1024, 2048], P('sp', 'tp')
- mid_grad: bfloat16 [1536, 2048], P('sp', 'tp')
- out_weight_grad: float32 [2048, 1024], P('sp', 'tp')
- input_grad: bfloat16 [1536, 1024], P('sp', 'tp')
- out_gate_grad: bfloat16 [1536, 1024], P('sp', 'tp')
- in_gate_grad: bfloat16 [1536, 1024], P('sp', 'tp')
The draws below stay inside these ranges and needn't reach their ends.
Inputs may be any that keep to these rules, and one draw needn't show every extreme that they name: `routes`: each token names 2 different experts; within each aligned block of 192 tokens no expert is named by more than 96 tokens, a bound that some block reaches.
All inputs are finite; a program needn't handle non-finite values.
Results may differ from the reference program's by a relative error of at most 0.014.
Values may be sent and summed in bfloat16 or wider, within the bound.
A program may use at most 64 MiB of HBM per device.

```python
import math
import jax
import jax.numpy as jnp
import numpy as np
from jax import lax

D = 2048
CHANNELS = 1024
FF = 1024
TOP_K = 2
TAPS = 3
EXP_DEV = 1
TOK_DEV = 192
EXPERTS = 8
TOKENS = 1536
CAP = 96
N_SP = 8
N_TP = 4


def with_spikes(result, key, source, target, parts, factor):
    def block_of(dim):
        return (jnp.arange(result.shape[dim]) // (result.shape[dim] // parts)).reshape((-1,) + (1,) * (result.ndim - 1 - dim))

    near = jax.random.permutation(key, parts)[block_of(target)]
    far = (block_of(target) + parts // 2) % parts
    return jnp.where((block_of(source) == near) | (block_of(source) == far), factor * result, result)


def levels(stream_key, shape, shards, least, top_value):
    def one(position, parts):
        heights = jax.random.uniform(jax.random.fold_in(jax.random.fold_in(stream_key, 6), position), (parts,), jnp.float32, least / len(shards), top_value / len(shards))
        return jnp.repeat(jnp.exp(heights), shape[position] // parts).reshape((-1,) + (1,) * (len(shape) - position - 1))

    loudness = one(*shards[0])
    for cut in shards[1:]:
        loudness = loudness * one(*cut)
    return loudness


def shared_out(stream_key, own, number, rows, count, top, bound, slope):
    ranking = jax.random.permutation(stream_key, count)
    packed, usual = load_shares(count, rows * top, bound, slope, True), load_shares(count, rows * top, bound, slope, False)
    places = jnp.arange(count)

    def named(tallies, offset_by):
        used = int((tallies > 0).sum())
        fixed = max(1, used // 4)
        shifted = fixed + (places - fixed + offset_by * (used - fixed)) % max(1, count - fixed)
        return jnp.zeros((count,), jnp.int32).at[ranking[jnp.where(places < fixed, places, shifted)]].set(jnp.asarray(tallies, jnp.int32))

    tallies = jnp.where(number % 4 == 0, named(packed, number // 4), named(usual, number - number // 4 - 1))
    mixed = jax.random.permutation(jax.random.fold_in(own, 3), count)
    giver, receiver = mixed[0:count // 2 * 2:2], mixed[1:count // 2 * 2:2]
    margin = jnp.minimum(tallies[giver] - 1, bound - tallies[receiver]) // 2
    margin = jnp.where((giver == ranking[0]) | (receiver == ranking[0]) | (tallies[receiver] == 0), 0, jnp.maximum(margin, 0))
    shifted = jax.random.randint(jax.random.fold_in(own, 4), (count // 2,), 0, 1 << 20) % (margin + 1)
    tallies = tallies.at[giver].add(-shifted).at[receiver].add(shifted)
    members = jnp.searchsorted(jnp.cumsum(tallies), jnp.arange(rows * top), side="right").astype(jnp.int32)
    listing = members.reshape(top, rows).T
    listing = listing[jax.random.permutation(jax.random.fold_in(own, 1), rows)]
    offset_by = jax.random.randint(jax.random.fold_in(own, 2), (rows, 1), 0, top)
    return jnp.take_along_axis(listing, (jnp.arange(top)[None, :] + offset_by) % top, axis=1)


def load_shares(amount, total, reach, lean, full):
    loads = [(1 << 20) // math.isqrt(grade ** lean) + 1 for grade in range(1, amount + 1)]
    largest = reach if full else min(reach, max(-(-total // amount), total * loads[0] // sum(loads)))
    least = 1 if total - largest >= amount - 1 else 0
    holding, surplus = [largest] + [least] * (amount - 1), total - largest - least * (amount - 1)
    while surplus > 0:
        free = [i for i in range(1, amount) if holding[i] < largest] or [i for i in range(1, amount) if holding[i] < reach]
        mass, remaining = sum([loads[i] for i in free]), surplus
        for i in free:
            addition = min(reach - holding[i], max(1, remaining * loads[i] // mass), surplus)
            holding[i] = holding[i] + addition
            surplus = surplus - addition
    return np.array(holding)


def scatter_about(key, shape, scale, limit, cuts=(), kind=jnp.bfloat16):
    factor_of = levels(key, shape, cuts, -0.22, 0.18) if cuts else 1.0
    result = jax.random.normal(key, shape, jnp.float32) * scale * factor_of
    return jnp.minimum(jnp.maximum(result, -limit), limit).astype(kind)


def gaussian_with(stream_key, extent, spread, bound, pieces, heavy, held_as=jnp.bfloat16):
    entries = spread * jax.random.normal(stream_key, extent, jnp.float32)
    if pieces:
        entries = entries * levels(stream_key, extent, pieces, -0.22, 0.18)
    return jnp.clip(with_spikes(entries, jax.random.fold_in(stream_key, 3), *heavy), -bound, bound).astype(held_as)


def setup_inputs(seed: int = 0) -> dict:
    streams_of = jax.random.split(jax.random.key(seed), 13)
    out_grad = gaussian_with(streams_of[0], (TOKENS, D), 1.0, 6.0, ((0, 8),), (0, 1, 8, 2.0))
    routes_keys = jax.random.split(jax.random.fold_in(streams_of[1], 1), TOKENS // TOK_DEV)
    routes_turns = jax.random.permutation(jax.random.fold_in(streams_of[1], 3), TOKENS // TOK_DEV)
    routes = jax.vmap(lambda own, number: shared_out(jax.random.fold_in(streams_of[1], 2), own, number, TOK_DEV, EXPERTS, TOP_K, CAP, 1))(routes_keys, routes_turns).reshape((TOKENS, TOP_K))
    route_weight = jnp.clip(0.3 + 1.2 * jax.random.uniform(streams_of[2], (TOKENS, TOP_K), jnp.float32) ** levels(streams_of[2], (TOKENS, TOP_K), ((0, 8),), -0.2, 0.2), 0.3, 1.5)
    expert_rows = scatter_about(streams_of[3], (EXPERTS // EXP_DEV, EXPERTS, CAP, D), 1.0, 6.0, ((1, 8),))
    gate_weight = scatter_about(streams_of[4], (EXPERTS, D, FF), D ** -0.5, 0.125, ((0, 8), (2, 4)))
    up_weight = scatter_about(streams_of[5], (EXPERTS, D, FF), D ** -0.5, 0.125, ((0, 8), (2, 4)))
    down_weight = scatter_about(streams_of[6], (EXPERTS, FF, D), FF ** -0.5, 0.1875, ((0, 8), (1, 4)))
    conv_input = scatter_about(streams_of[7], (TOKENS, CHANNELS), 1.0, 6.0, ((0, 8), (1, 4)))
    out_gate = scatter_about(streams_of[8], (TOKENS, CHANNELS), 1.0, 6.0, ((0, 8), (1, 4)))
    in_gate = scatter_about(streams_of[9], (TOKENS, CHANNELS), 1.0, 6.0, ((0, 8), (1, 4)))
    taps = scatter_about(streams_of[10], (TAPS, CHANNELS), 0.6, 3.0, ((1, 4),), jnp.float32)
    out_weight = scatter_about(streams_of[11], (D, CHANNELS), CHANNELS ** -0.5, 0.1875, ((1, 4),))
    return {"out_grad": out_grad, "routes": routes, "route_weight": route_weight, "expert_rows": expert_rows, "gate_weight": gate_weight, "up_weight": up_weight, "down_weight": down_weight, "conv_input": conv_input, "out_gate": out_gate, "in_gate": in_gate, "taps": taps, "out_weight": out_weight}


def slot_layout(routes):
    flat = routes.reshape(N_SP, TOK_DEV * TOP_K)
    onehot = (flat[:, :, None] == jnp.arange(EXPERTS, dtype=jnp.int32)[None, None, :]).astype(jnp.int32)
    before = jnp.cumsum(onehot, axis=1) - onehot
    place = jnp.sum(before * onehot, axis=2).astype(jnp.int32)
    source = jnp.broadcast_to(jnp.arange(N_SP, dtype=jnp.int32)[:, None], flat.shape)
    return flat, place, source


def one_expert(operands):
    rows, grads, w_gate, w_up, w_down = operands
    rows = rows.reshape(-1, D)
    grads = grads.reshape(-1, D)
    gate = jnp.dot(rows, w_gate, preferred_element_type=jnp.float32)
    up = jnp.dot(rows, w_up, preferred_element_type=jnp.float32)
    sig = jax.nn.sigmoid(gate)
    act = (gate * sig * up).astype(jnp.bfloat16)
    act_grad = jnp.dot(grads, w_down.T, preferred_element_type=jnp.float32)
    up_part = (act_grad * gate * sig).astype(jnp.bfloat16)
    gate_part = (act_grad * up * sig * (1.0 + gate * (1.0 - sig))).astype(jnp.bfloat16)
    down_g = jnp.dot(act.T, grads, preferred_element_type=jnp.float32).astype(jnp.bfloat16)
    gate_g = jnp.dot(rows.T, gate_part, preferred_element_type=jnp.float32).astype(jnp.bfloat16)
    up_g = jnp.dot(rows.T, up_part, preferred_element_type=jnp.float32).astype(jnp.bfloat16)
    group = FF // N_TP
    total = jnp.zeros((rows.shape[0], D), jnp.float32)
    for index in range(N_TP):
        lower = index * group
        upper = lower + group
        part = jnp.dot(gate_part[:, lower:upper], w_gate[:, lower:upper].T, preferred_element_type=jnp.float32)
        part = part + jnp.dot(up_part[:, lower:upper], w_up[:, lower:upper].T, preferred_element_type=jnp.float32)
        rounded = lax.optimization_barrier(part.astype(jnp.bfloat16))
        total = total + rounded.astype(jnp.float32)
    row_grad = total.astype(jnp.bfloat16).reshape(N_SP, CAP, D)
    return gate_g, up_g, down_g, row_grad


def reference(out_grad, routes, route_weight, expert_rows, gate_weight, up_weight, down_weight,
              conv_input, out_gate, in_gate, taps, out_weight):
    flat, place, source = slot_layout(routes)
    slot_grad = (route_weight[:, :, None] * out_grad[:, None, :].astype(jnp.float32)).astype(jnp.bfloat16)
    slot_grad = slot_grad.reshape(N_SP, TOK_DEV * TOP_K, D)
    expert_grads = jnp.zeros((N_SP, EXPERTS, CAP, D), jnp.bfloat16).at[source, flat, place].set(slot_grad)
    rows_by_expert = jnp.moveaxis(expert_rows, 1, 0)
    grads_by_expert = jnp.moveaxis(expert_grads, 1, 0)
    gate_grad, up_grad, down_grad, row_grad = lax.map(
        one_expert, (rows_by_expert, grads_by_expert, gate_weight, up_weight, down_weight))
    picked = row_grad[flat, source, place].astype(jnp.float32)
    picked = picked.reshape(TOKENS, TOP_K, D).sum(axis=1)
    mid_grad = (out_grad.astype(jnp.float32) + picked).astype(jnp.bfloat16)
    mixed = in_gate.astype(jnp.float32) * conv_input.astype(jnp.float32)
    padded = jnp.concatenate([jnp.zeros((TAPS - 1, CHANNELS), jnp.float32), mixed], axis=0)
    conv = jnp.zeros_like(mixed)
    for tap in range(TAPS):
        conv = conv + taps[tap][None, :] * padded[TAPS - 1 - tap:TAPS - 1 - tap + TOKENS]
    gated = (out_gate.astype(jnp.float32) * conv).astype(jnp.bfloat16)
    out_weight_grad = jnp.dot(mid_grad.T, gated, preferred_element_type=jnp.float32)
    gated_grad = jnp.dot(mid_grad, out_weight, preferred_element_type=jnp.float32)
    out_gate_grad = (gated_grad * conv).astype(jnp.bfloat16)
    conv_grad = gated_grad * out_gate.astype(jnp.float32)
    after = jnp.concatenate([conv_grad, jnp.zeros((TAPS - 1, CHANNELS), jnp.float32)], axis=0)
    mixed_grad = jnp.zeros_like(conv_grad)
    for tap in range(TAPS):
        mixed_grad = mixed_grad + taps[tap][None, :] * after[tap:tap + TOKENS]
    input_grad = (mixed_grad * in_gate.astype(jnp.float32)).astype(jnp.bfloat16)
    in_gate_grad = (mixed_grad * conv_input.astype(jnp.float32)).astype(jnp.bfloat16)
    return (gate_grad, up_grad, down_grad, mid_grad, out_weight_grad,
            input_grad, out_gate_grad, in_gate_grad)
```

```python
import functools

import jax
import jax.numpy as jnp
from jax import lax
from jax.experimental import pallas as pl
from jax.experimental.pallas import tpu as pltpu
from jax.sharding import PartitionSpec as P

ANY_SPEC = pl.BlockSpec(memory_space=pl.ANY)
VMEM_SPEC = pl.BlockSpec(memory_space=pltpu.VMEM)


def passed_along(shard, axis, by):
    peers = lax.axis_size(axis)
    pairs = [(i, i + by) for i in range(peers) if 0 <= i + by < peers]
    return lax.ppermute(shard, axis, pairs)


def remote(src, dst, send_sem, recv_sem, **target):
    return pltpu.make_async_remote_copy(
        src_ref=src,
        dst_ref=dst,
        send_sem=send_sem,
        recv_sem=recv_sem,
        device_id=target,
        device_id_type=pl.DeviceIdType.MESH,
    )


def greet(sp_peers, tp_peers):
    barrier = pltpu.get_barrier_semaphore()
    for peer in sp_peers:
        pl.semaphore_signal(
            barrier, inc=1, device_id={"sp": peer}, device_id_type=pl.DeviceIdType.MESH
        )
    for peer in tp_peers:
        pl.semaphore_signal(
            barrier, inc=1, device_id={"tp": peer}, device_id_type=pl.DeviceIdType.MESH
        )
    pl.semaphore_wait(barrier, len(sp_peers) + len(tp_peers))


def tp_places(groups):
    member = lax.axis_index("tp")
    sibling = member + 1 - 2 * lax.rem(member, 2)
    others = [lax.rem(member + 2 * d, groups) for d in range(1, groups // 2)]
    return member, sibling, others


def columns(member, share):
    return pl.ds(pl.multiple_of(member * share, share), share)


def spread_kernel(
    n,
    groups,
    send_ref,
    rows_hbm,
    wg_hbm,
    wu_hbm,
    out_ref,
    gate_ref,
    up_ref,
    rows_ref,
    wg_ref,
    wu_ref,
    load_sem,
    own_sem,
    s_a,
    r_a,
    s_f,
    r_f,
    s_g,
    r_g,
):
    me = lax.axis_index("sp")
    member, sibling, others = tp_places(groups)
    share = send_ref.shape[2]
    greet([lax.rem(me + off, n) for off in range(1, n)], [sibling] + others)

    def across(off):
        dest = lax.rem(me + off, n)
        return remote(
            send_ref.at[dest],
            out_ref.at[me, :, columns(member, share)],
            s_a.at[off],
            r_a.at[off],
            sp=dest,
        )

    def block(off, owner):
        return out_ref.at[lax.rem(me + n - off, n), :, columns(owner, share)]

    def hand(off, d):
        target = sibling if d == 0 else others[d - 1]
        return remote(
            block(off, member), block(off, member), s_f.at[d, off], r_f.at[d, off], tp=target
        )

    def relay(off, d):
        piece = block(off, others[d - 1])
        return remote(piece, piece, s_g.at[d - 1, off], r_g.at[d - 1, off], tp=sibling)

    def hand_on(off):
        for d in range(groups // 2):
            hand(off, d).start()

    def relay_on(off):
        for d in range(1, groups // 2):
            hand(off, d).wait_recv()
            relay(off, d).start()

    own = pltpu.make_async_copy(send_ref.at[me], out_ref.at[me, :, columns(member, share)], own_sem)
    own.start()

    def send_out(off, carry):
        across(off).start()
        return carry

    lax.fori_loop(1, n, send_out, 0)
    loads = [
        pltpu.make_async_copy(wg_hbm, wg_ref, load_sem.at[0]),
        pltpu.make_async_copy(wu_hbm, wu_ref, load_sem.at[1]),
        pltpu.make_async_copy(rows_hbm, rows_ref, load_sem.at[2]),
    ]
    for load in loads:
        load.start()
    own.wait()
    hand_on(0)
    tall = rows_ref.shape[0]
    inside = (tall // n) % 16 == 0
    pieces = n if inside else 4
    size = tall // pieces

    def project(piece):
        at = pl.ds(pl.multiple_of(piece * size, size), size)
        rows = rows_ref[at, :]
        gate_ref[at, :] = jnp.dot(rows, wg_ref[...], preferred_element_type=jnp.float32)
        up_ref[at, :] = jnp.dot(rows, wu_ref[...], preferred_element_type=jnp.float32)

    def project_step(piece, carry):
        project(piece)
        return carry

    for load in loads:
        load.wait()
    if inside:
        project(n - 1)
    else:
        lax.fori_loop(0, pieces, project_step, 0)

    def step(off, carry):
        across(off).wait_recv()
        hand_on(off)
        relay_on(off - 1)
        if inside:
            project(off - 1)
        return carry

    lax.fori_loop(1, n, step, 0)
    relay_on(n - 1)

    def finish(off, carry):
        hand(off, 0).wait_recv()
        for d in range(groups // 2):
            hand(off, d).wait_send()
        for d in range(1, groups // 2):
            relay(off, d).wait()
        return carry

    lax.fori_loop(0, n, finish, 0)

    def drain(off, carry):
        across(off).wait_send()
        return carry

    lax.fori_loop(1, n, drain, 0)


def spread(blocks, rows, gate_weight, up_weight, groups):
    n, depth, share = blocks.shape
    hidden = jax.ShapeDtypeStruct((rows.shape[0], gate_weight.shape[1]), jnp.float32)
    dma = pltpu.SemaphoreType.DMA
    return pl.pallas_call(
        functools.partial(spread_kernel, n, groups),
        out_shape=(
            jax.ShapeDtypeStruct((n, depth, share * groups), blocks.dtype),
            hidden,
            hidden,
        ),
        in_specs=[VMEM_SPEC, ANY_SPEC, ANY_SPEC, ANY_SPEC],
        out_specs=(VMEM_SPEC, VMEM_SPEC, VMEM_SPEC),
        scratch_shapes=[
            pltpu.VMEM(rows.shape, rows.dtype),
            pltpu.VMEM(gate_weight.shape, gate_weight.dtype),
            pltpu.VMEM(up_weight.shape, up_weight.dtype),
            dma((3,)),
            dma(()),
            dma((n,)),
            dma((n,)),
            dma((groups // 2, n)),
            dma((groups // 2, n)),
            dma((groups // 2 - 1, n)),
            dma((groups // 2 - 1, n)),
        ],
        compiler_params=pltpu.CompilerParams(collective_id=0, has_side_effects=True),
    )(blocks, rows, gate_weight, up_weight)


def collect_kernel(
    n,
    groups,
    part_ref,
    rows_hbm,
    grads_hbm,
    act_hbm,
    gate_hbm,
    up_hbm,
    out_ref,
    gate_out,
    up_out,
    down_out,
    near,
    pair,
    far,
    final,
    rows_ref,
    grads_ref,
    act_ref,
    gate_ref,
    up_ref,
    load_sem,
    s_n,
    r_n,
    s_f,
    r_f,
    s_a,
    r_a,
):
    me = lax.axis_index("sp")
    member, sibling, others = tp_places(groups)
    half = groups // 2
    share = out_ref.shape[2]
    seat, row = lax.rem(member, 2), lax.div(member, 2)
    greet([lax.rem(me + off, n) for off in range(1, n)], [sibling] + others)

    def home(off):
        return lax.rem(me + off, n)

    def to_sibling(off, h):
        return remote(
            part_ref.at[home(off), :, columns(2 * h + 1 - seat, share)],
            near.at[home(off), h],
            s_n.at[h, off],
            r_n.at[h, off],
            tp=sibling,
        )

    def to_other(off, d):
        h = lax.rem(row + d, half)
        return remote(
            pair.at[home(off), h],
            far.at[d - 1, home(off)],
            s_f.at[d - 1, off],
            r_f.at[d - 1, off],
            tp=others[d - 1],
        )

    def to_home(off):
        return remote(
            final.at[home(off)], out_ref.at[me], s_a.at[off], r_a.at[off], sp=home(off)
        )

    def open_step(i, carry):
        off = lax.rem(i + 1, n)
        for h in range(half):
            to_sibling(off, h).start()
        return carry

    lax.fori_loop(0, n, open_step, 0)
    sources = (act_hbm, gate_hbm, up_hbm, rows_hbm, grads_hbm)
    held = (act_ref, gate_ref, up_ref, rows_ref, grads_ref)
    loads = [pltpu.make_async_copy(a, b, load_sem.at[i]) for i, (a, b) in enumerate(zip(sources, held))]
    for load in loads:
        load.start()
    width = rows_ref.shape[1]
    inside = width % (128 * n) == 0
    pieces = n if inside else 8
    size = width // pieces

    def across_rows(a, b):
        total = lax.dot_general(a, b, (((0,), (0,)), ((), ())), preferred_element_type=jnp.float32)
        return total.astype(jnp.bfloat16)

    def weigh(piece):
        at = columns(piece, size)
        rows = rows_ref[:, at]
        gate_out[at, :] = across_rows(rows, gate_ref[...])
        up_out[at, :] = across_rows(rows, up_ref[...])
        down_out[:, at] = across_rows(act_ref[...], grads_ref[:, at])

    def weigh_step(piece, carry):
        weigh(piece)
        return carry

    def pair_step(i, carry):
        off = lax.rem(i + 1, n)
        for h in range(half):
            to_sibling(off, h).wait_recv()
            mine = part_ref[home(off), :, columns(2 * h + seat, share)].astype(jnp.float32)
            total = mine + near[home(off), h].astype(jnp.float32)
            pair[home(off), h] = total.astype(jnp.bfloat16)
        for d in range(1, half):
            to_other(off, d).start()
        return carry

    lax.fori_loop(0, n, pair_step, 0)

    for load in loads:
        load.wait()
    if inside:
        weigh(n - 1)
    else:
        lax.fori_loop(0, pieces, weigh_step, 0)

    def summed(off):
        total = pair[home(off), row].astype(jnp.float32)
        for d in range(1, half):
            to_other(off, d).wait_recv()
            total = total + far[d - 1, home(off)].astype(jnp.float32)
        return total.astype(jnp.bfloat16)

    def home_step(off, carry):
        final[home(off)] = summed(off)
        to_home(off).start()
        if inside:
            weigh(off - 1)
        return carry

    lax.fori_loop(1, n, home_step, 0)
    out_ref[me] = summed(0)

    def drain(off, carry):
        for h in range(half):
            to_sibling(off, h).wait_send()
        for d in range(1, half):
            to_other(off, d).wait_send()
        return carry

    lax.fori_loop(0, n, drain, 0)

    def arrive(off, carry):
        to_home(off).wait()
        return carry

    lax.fori_loop(1, n, arrive, 0)


def collect(parts, rows, grads, act, gate_part, up_part, groups):
    n, depth, width = parts.shape
    ff = act.shape[1]
    share, half = width // groups, groups // 2
    dma = pltpu.SemaphoreType.DMA
    return pl.pallas_call(
        functools.partial(collect_kernel, n, groups),
        out_shape=(
            jax.ShapeDtypeStruct((n, depth, share), parts.dtype),
            jax.ShapeDtypeStruct((width, ff), parts.dtype),
            jax.ShapeDtypeStruct((width, ff), parts.dtype),
            jax.ShapeDtypeStruct((ff, width), parts.dtype),
        ),
        in_specs=[VMEM_SPEC] + [ANY_SPEC] * 5,
        out_specs=(VMEM_SPEC,) * 4,
        scratch_shapes=[
            pltpu.VMEM((n, half, depth, share), parts.dtype),
            pltpu.VMEM((n, half, depth, share), parts.dtype),
            pltpu.VMEM((half - 1, n, depth, share), parts.dtype),
            pltpu.VMEM((n, depth, share), parts.dtype),
            pltpu.VMEM(rows.shape, rows.dtype),
            pltpu.VMEM(grads.shape, grads.dtype),
            pltpu.VMEM(act.shape, act.dtype),
            pltpu.VMEM(act.shape, act.dtype),
            pltpu.VMEM(act.shape, act.dtype),
            dma((5,)),
            dma((half, n)),
            dma((half, n)),
            dma((half - 1, n)),
            dma((half - 1, n)),
            dma((n,)),
            dma((n,)),
        ],
        compiler_params=pltpu.CompilerParams(collective_id=1, has_side_effects=True),
    )(parts, rows, grads, act, gate_part, up_part)


def widen_kernel(groups, chunks, own_ref, out_ref, own_sem, s_f, r_f, s_g, r_g):
    member, sibling, others = tp_places(groups)
    rows, share = own_ref.shape
    size = rows // chunks
    greet([], [sibling] + others)

    def place(c, owner):
        return out_ref.at[pl.ds(c * size, size), columns(owner, share)]

    def hand(c, d):
        target = sibling if d == 0 else others[d - 1]
        return remote(
            own_ref.at[pl.ds(c * size, size)],
            place(c, member),
            s_f.at[d, c],
            r_f.at[d, c],
            tp=target,
        )

    def relay(c, d):
        piece = place(c, others[d - 1])
        return remote(piece, piece, s_g.at[d - 1, c], r_g.at[d - 1, c], tp=sibling)

    for c in range(chunks):
        for d in range(1, groups // 2):
            hand(c, d).start()
    for c in range(chunks):
        hand(c, 0).start()
    own = pltpu.make_async_copy(own_ref, out_ref.at[:, columns(member, share)], own_sem)
    own.start()
    for c in range(chunks):
        for d in range(1, groups // 2):
            hand(c, d).wait_recv()
            relay(c, d).start()
    own.wait()
    for c in range(chunks):
        hand(c, 0).wait_recv()
        for d in range(groups // 2):
            hand(c, d).wait_send()
        for d in range(1, groups // 2):
            relay(c, d).wait()


def widen(own, groups):
    rows, share = own.shape
    chunks = 4 if rows % 64 == 0 else 1
    dma = pltpu.SemaphoreType.DMA
    return pl.pallas_call(
        functools.partial(widen_kernel, groups, chunks),
        out_shape=jax.ShapeDtypeStruct((rows, share * groups), own.dtype),
        in_specs=[VMEM_SPEC],
        out_specs=VMEM_SPEC,
        scratch_shapes=[
            dma(()),
            dma((groups // 2, chunks)),
            dma((groups // 2, chunks)),
            dma((groups // 2 - 1, chunks)),
            dma((groups // 2 - 1, chunks)),
        ],
        compiler_params=pltpu.CompilerParams(collective_id=2, has_side_effects=True),
    )(own)


def fold_kernel(n, part_ref, out_ref, near, pair, far, s_n, r_n, s_f, r_f):
    me = lax.axis_index("sp")
    seat, row = lax.rem(me, 2), lax.div(me, 2)
    partner = me + 1 - 2 * seat
    half = n // 2
    greet([partner] + [lax.rem(me + 2 * d, n) for d in range(1, half)], [])

    def spot(d):
        return lax.rem(row + d, half)

    def to_partner(d):
        return remote(
            part_ref.at[2 * spot(d) + 1 - seat], near.at[d], s_n.at[d], r_n.at[d], sp=partner
        )

    def to_owner(d):
        return remote(
            pair.at[d], far.at[d], s_f.at[d], r_f.at[d], sp=lax.rem(me + 2 * d, n)
        )

    def open_step(i, carry):
        to_partner(lax.rem(i + 1, half)).start()
        return carry

    lax.fori_loop(0, half, open_step, 0)

    def paired(d):
        to_partner(d).wait_recv()
        mine = part_ref[2 * spot(d) + seat].astype(jnp.float32)
        return mine + near[d].astype(jnp.float32)

    def pair_step(d, carry):
        pair[d] = paired(d).astype(jnp.bfloat16)
        to_owner(d).start()
        return carry

    lax.fori_loop(1, half, pair_step, 0)
    out_ref[...] = paired(0)

    def add_step(d, carry):
        to_owner(d).wait_recv()
        out_ref[...] += far[d].astype(jnp.float32)
        return carry

    lax.fori_loop(1, half, add_step, 0)

    def drain(d, carry):
        to_partner(d).wait_send()
        return carry

    lax.fori_loop(0, half, drain, 0)

    def drain_owner(d, carry):
        to_owner(d).wait_send()
        return carry

    lax.fori_loop(1, half, drain_owner, 0)


def fold(parts):
    n, rows, cols = parts.shape
    half = n // 2
    dma = pltpu.SemaphoreType.DMA
    return pl.pallas_call(
        functools.partial(fold_kernel, n),
        out_shape=jax.ShapeDtypeStruct((rows, cols), jnp.float32),
        in_specs=[VMEM_SPEC],
        out_specs=VMEM_SPEC,
        scratch_shapes=[
            pltpu.VMEM((half, rows, cols), parts.dtype),
            pltpu.VMEM((half, rows, cols), parts.dtype),
            pltpu.VMEM((half, rows, cols), parts.dtype),
            dma((half,)),
            dma((half,)),
            dma((half,)),
            dma((half,)),
        ],
        compiler_params=pltpu.CompilerParams(collective_id=3, has_side_effects=True),
    )(parts)


BF16, F32 = jnp.bfloat16, jnp.float32


def dot_nn(a, b):
    return jnp.dot(a, b, preferred_element_type=F32)


def dot_nt(a, b):
    return lax.dot_general(a, b, (((1,), (1,)), ((), ())), preferred_element_type=F32)


def dot_tn(a, b):
    return lax.dot_general(a, b, (((0,), (0,)), ((), ())), preferred_element_type=F32)


def fused_kernel(
    n,
    groups,
    out_grad,
    routes,
    route_weight,
    conv_input,
    out_gate,
    in_gate,
    taps,
    rows_hbm,
    wg_hbm,
    wu_hbm,
    dn_hbm,
    ow_hbm,
    gate_out,
    up_out,
    down_out,
    mid_out,
    weight_out,
    input_out,
    out_gate_out,
    in_gate_out,
    rows,
    wgu,
    dn,
    ow,
    hidden,
    place,
    weight,
    picker,
    send,
    grads,
    act,
    parts,
    row_part,
    near,
    pair,
    far,
    final,
    back,
    total,
    wide,
    rim,
    mixed,
    conv,
    gated,
    slices,
    follow,
    later,
    load_sem,
    s_a,
    r_a,
    s_x,
    r_x,
    s_b,
    r_b,
    s_g,
    r_g,
    s_n,
    r_n,
    s_f,
    r_f,
    s_h,
    r_h,
    s_rim,
    r_rim,
    s_d,
    r_d,
    s_p,
    r_p,
    s_m,
    r_m,
    s_mx,
    r_mx,
    s_mr,
    r_mr,
    s_v,
    r_v,
    s_w,
    r_w,
    s_l,
    r_l,
):
    me = lax.axis_index("sp")
    member = lax.axis_index("tp")
    seat = lax.rem(member, 2)
    line = lax.div(member, 2)
    sibling = member + 1 - 2 * seat
    other = lax.rem(member + 2, groups)
    tokens, width = out_grad.shape
    slots = rows.shape[1]
    ff = dn.shape[0]
    share = width // groups
    deep = n // 2
    per = n // groups
    span = width // n

    barrier = pltpu.get_barrier_semaphore()

    def call(off, carry):
        pl.semaphore_signal(
            barrier,
            inc=1,
            device_id={"sp": lax.rem(me + off, n)},
            device_id_type=pl.DeviceIdType.MESH,
        )
        return carry

    lax.fori_loop(1, n, call, 0)
    for peer in (sibling, other):
        pl.semaphore_signal(
            barrier, inc=1, device_id={"tp": peer}, device_id_type=pl.DeviceIdType.MESH
        )
    loads = [
        pltpu.make_async_copy(wg_hbm, wgu.at[:, pl.ds(0, ff)], load_sem.at[0]),
        pltpu.make_async_copy(wu_hbm, wgu.at[:, pl.ds(ff, ff)], load_sem.at[1]),
        pltpu.make_async_copy(rows_hbm, rows, load_sem.at[2]),
        pltpu.make_async_copy(dn_hbm, dn, load_sem.at[3]),
        pltpu.make_async_copy(ow_hbm, ow, load_sem.at[4]),
    ]
    for load in loads:
        load.start()

    def shift(k, way):
        q = lax.div(k, 2)
        step = lax.div(q + 1, 2) * (2 * lax.rem(q, 2) - 1) * way
        deeper = lax.rem(lax.div(me, 2) + step + deep, deep)
        side = lax.rem(lax.rem(me, 2) + lax.rem(k, 2), 2)
        return 2 * deeper + side

    def dest(k):
        return shift(k, 1)

    def source(k):
        return shift(k, -1)

    def slice_at(j):
        return pl.ds(pl.multiple_of(j * span, span), span)

    def across(k):
        return remote(
            send.at[dest(k)],
            grads.at[me, :, columns(member, share)],
            s_a.at[k],
            r_a.at[k],
            sp=dest(k),
        )

    def hand(k):
        piece = grads.at[source(k), :, columns(member, share)]
        return remote(piece, piece, s_b.at[k], r_b.at[k], tp=sibling)

    def cross(k):
        piece = grads.at[source(k), :, columns(member, share)]
        return remote(piece, piece, s_x.at[k], r_x.at[k], tp=other)

    def relay(k):
        piece = grads.at[source(k), :, columns(other, share)]
        return remote(piece, piece, s_g.at[k], r_g.at[k], tp=sibling)

    def to_sibling(k, h):
        return remote(
            row_part.at[source(k), :, columns(2 * h + 1 - seat, share)],
            near.at[source(k), h],
            s_n.at[h, k],
            r_n.at[h, k],
            tp=sibling,
        )

    def to_other(k):
        return remote(
            pair.at[source(k), 1 - line], far.at[source(k)], s_f.at[k], r_f.at[k], tp=other
        )

    def to_home(k):
        return remote(final.at[source(k)], back.at[me], s_h.at[k], r_h.at[k], sp=source(k))

    def rim_copy(i, ref):
        return remote(
            ref.at[pl.ds(tokens - 16, 16)],
            rim.at[i],
            s_rim.at[i],
            r_rim.at[i],
            sp=lax.rem(me + 1, n),
        )

    def gated_along(q):
        return remote(gated.at[me], gated.at[me], s_d.at[q], r_d.at[q], sp=dest(2 * q))

    def gated_over(q):
        piece = gated.at[source(2 * q)]
        return remote(piece, piece, s_p.at[q], r_p.at[q], sp=dest(1))

    names = lax.broadcasted_iota(jnp.int32, (n, tokens), 0)
    chosen = jnp.zeros((n, tokens), jnp.bool_)
    weights = jnp.zeros((n, tokens), F32)
    for choice in range(routes.shape[0]):
        named = names == routes[choice : choice + 1, :]
        chosen = jnp.logical_or(chosen, named)
        weights = weights + jnp.where(named, route_weight[choice : choice + 1, :], 0.0)
    first = lax.broadcasted_iota(jnp.int32, (tokens, tokens), 0)
    second = lax.broadcasted_iota(jnp.int32, (tokens, tokens), 1)
    earlier = jnp.where(first < second, 1.0, 0.0).astype(BF16)
    marks = jnp.where(chosen, 1.0, 0.0)
    places = jnp.where(chosen, dot_nn(marks.astype(BF16), earlier), -1.0)
    for e in range(n):
        place[e] = places[e : e + 1, :]
        weight[e] = weights[e : e + 1, :]
    seats = lax.broadcasted_iota(jnp.int32, (slots, tokens), 0).astype(F32)

    def pick(e):
        filled = place[e] == seats
        found = jnp.where(filled, 1.0, 0.0).astype(BF16)
        picker[e] = found
        held = jnp.sum(jnp.where(filled, weight[e], 0.0), axis=1, keepdims=True)
        return found, held

    pl.semaphore_wait(barrier, n + 1)
    for i, ref in enumerate((in_gate, conv_input)):
        rim_copy(i, ref).start()

    def build(k, carry):
        e = dest(k)
        found, held = pick(e)
        own = dot_nn(found, out_grad[:, columns(member, share)])
        send[e] = (held * own).astype(BF16)
        across(k).start()
        return carry

    lax.fori_loop(1, n, build, 0)
    found, held = pick(me)
    for g in range(groups):
        at = pl.ds(g * share, share)
        grads[me, :, at] = (held * dot_nn(found, out_grad[:, at])).astype(BF16)
    for load in loads[:3]:
        load.wait()
    couples = 2

    def project(c, carry):
        at = pl.ds(c * couples, couples)
        rows_c = rows[at].reshape(couples * slots, width)
        hidden[at] = dot_nn(rows_c, wgu[...]).reshape(couples, slots, 2 * ff)
        return carry

    lax.fori_loop(0, n // couples, project, 0)

    for i, ref in enumerate((in_gate, conv_input)):
        rim_copy(i, ref).wait_recv()
    prior = rim[0].astype(F32) * rim[1].astype(F32)
    mixed[0:16] = jnp.where(me == 0, 0.0, prior)
    mixed[pl.ds(16, tokens)] = in_gate[...].astype(F32) * conv_input[...].astype(F32)
    reach = taps.shape[0]
    conv_sum = taps[0:1, :] * mixed[pl.ds(16, tokens)]
    for tap in range(1, reach):
        conv_sum = conv_sum + taps[tap : tap + 1, :] * mixed[pl.ds(16 - tap, tokens)]
    conv[...] = conv_sum
    gated[me] = (out_gate[...].astype(F32) * conv_sum).astype(BF16)
    for q in range(1, deep):
        gated_along(q).start()
    gated_over(0).start()
    loads[3].wait()
    loads[4].wait()

    def arrive(k):
        across(k).wait_recv()
        cross(k).start()
        hand(k).start()

    def pass_on(k):
        cross(k).wait_recv()
        relay(k).start()

    def backward(k):
        @pl.when(k > 0)
        def _():
            hand(k).wait_recv()
            relay(k).wait_recv()

        s = source(k)
        gate = hidden[s, :, 0:ff]
        up = hidden[s, :, ff : 2 * ff]
        sig = jax.nn.sigmoid(gate)
        act[s] = (gate * sig * up).astype(BF16)
        act_grad = dot_nt(grads[s], dn[...])
        parts[s, :, 0:ff] = (act_grad * up * sig * (1.0 + gate * (1.0 - sig))).astype(BF16)
        parts[s, :, ff : 2 * ff] = (act_grad * gate * sig).astype(BF16)
        both = parts[s]
        for g in range(groups):
            at = pl.ds(g * share, share)
            row_part[s, :, at] = dot_nt(both, wgu[at, :]).astype(BF16)
        for h in range(2):
            to_sibling(k, h).start()

    def pair_up(k):
        s = source(k)
        for h in range(2):
            to_sibling(k, h).wait_recv()
            mine = row_part[s, :, columns(2 * h + seat, share)].astype(F32)
            pair[s, h] = (mine + near[s, h].astype(F32)).astype(BF16)
        to_other(k).start()

    def finish(k):
        s = source(k)
        to_other(k).wait_recv()
        final[s] = (pair[s, line].astype(F32) + far[s].astype(F32)).astype(BF16)

        @pl.when(k > 0)
        def _():
            to_home(k).start()

    def within(k, low, act_on):
        @pl.when(jnp.logical_and(k >= low, k < n))
        def _():
            act_on(k)

    def step(j, carry):
        within(j + 1, 1, arrive)
        within(j, 1, pass_on)
        within(j - 1, 0, backward)
        within(j - 2, 0, pair_up)
        within(j - 3, 0, finish)
        return carry

    lax.fori_loop(0, n + 3, step, 0)

    for q in range(1, deep):
        gated_along(q).wait_recv()
        gated_over(q).start()

    total[...] = out_grad[:, columns(member, share)].astype(F32) + dot_tn(picker[me], final[me])

    def gather_home(k, carry):
        e = dest(k)
        to_home(k).wait_recv()
        total[...] += dot_tn(picker[e], back[e])
        return carry

    lax.fori_loop(1, n, gather_home, 0)
    mid = total[...].astype(BF16)
    mid_out[...] = mid
    wide[:, columns(member, share)] = mid

    def mid_sibling():
        piece = wide.at[:, columns(member, share)]
        return remote(piece, piece, s_m, r_m, tp=sibling)

    def mid_other(q):
        piece = wide.at[:, slice_at(member * per + q)]
        return remote(piece, piece, s_mx.at[q], r_mx.at[q], tp=other)

    def mid_relay(q):
        piece = wide.at[:, slice_at(other * per + q)]
        return remote(piece, piece, s_mr.at[q], r_mr.at[q], tp=sibling)

    def slice_out(j):
        return remote(wide.at[:, slice_at(j)], slices.at[me], s_v.at[j], r_v.at[me], sp=j)

    def slice_in(s):
        return remote(wide.at[:, slice_at(me)], slices.at[s], s_v.at[s], r_v.at[s], sp=s)

    def slice_relay(s):
        piece = slices.at[s]
        return remote(piece, piece, s_w.at[s], r_w.at[s], tp=sibling)

    def send_slice(j):
        @pl.when(j != me)
        def _():
            slice_out(j).start()

    for q in range(per):
        mid_other(q).start()
    mid_sibling().start()
    for q in range(per):
        send_slice(member * per + q)

    chunk = 128 if width % 256 else 256
    chunks = width // chunk

    def weigh(piece, carry):
        at = columns(piece, chunk)
        tall = n * slots
        grown = dot_tn(rows[:, :, at].reshape(tall, chunk), parts[...].reshape(tall, 2 * ff))
        gate_out[at, :] = grown[:, 0:ff].astype(BF16)
        up_out[at, :] = grown[:, ff : 2 * ff].astype(BF16)
        down_out[:, at] = dot_tn(
            act[...].reshape(tall, ff), grads[:, :, at].reshape(tall, chunk)
        ).astype(BF16)
        return carry

    lax.fori_loop(0, chunks // 2, weigh, 0)
    for q in range(per):
        mid_other(q).wait_recv()
        mid_relay(q).start()
        send_slice(other * per + q)
    lax.fori_loop(chunks // 2, chunks, weigh, 0)
    mid_sibling().wait_recv()
    for q in range(per):
        mid_relay(q).wait_recv()
    gated_grad = dot_nn(wide[...], ow[...])
    conv_grad = gated_grad * out_gate[...].astype(F32)
    follow[pl.ds(0, tokens)] = conv_grad

    back_rim = remote(
        follow.at[pl.ds(0, 8)], later, s_l, r_l, sp=lax.rem(me + n - 1, n)
    )
    back_rim.start()
    out_gate_out[...] = (gated_grad * conv[...]).astype(BF16)
    for q in range(deep):
        gated_over(q).wait_recv()
    weight_out[...] = dot_tn(wide[:, slice_at(me)], gated[me])
    holder = lax.rem(lax.div(me, per), 2)

    def meet(off, carry):
        s = lax.rem(me + off, n)

        @pl.when(holder == seat)
        def _():
            slice_in(s).wait_recv()
            slice_relay(s).start()

        @pl.when(holder != seat)
        def _():
            slice_relay(s).wait_recv()

        weight_out[...] += dot_tn(slices[s], gated[s])
        return carry

    lax.fori_loop(1, n, meet, 0)
    back_rim.wait_recv()
    follow[pl.ds(tokens, 8)] = jnp.where(me == n - 1, 0.0, later[...])
    mixed_grad = taps[0:1, :] * follow[pl.ds(0, tokens)]
    for tap in range(1, reach):
        mixed_grad = mixed_grad + taps[tap : tap + 1, :] * follow[pl.ds(tap, tokens)]
    input_out[...] = (mixed_grad * in_gate[...].astype(F32)).astype(BF16)
    in_gate_out[...] = (mixed_grad * conv_input[...].astype(F32)).astype(BF16)

    def drain(k, carry):
        @pl.when(k > 0)
        def _():
            across(k).wait_send()
            hand(k).wait_send()
            cross(k).wait_send()
            relay(k).wait_send()
            to_home(k).wait_send()

        for h in range(2):
            to_sibling(k, h).wait_send()
        to_other(k).wait_send()
        return carry

    lax.fori_loop(0, n, drain, 0)

    def drain_slices(off, carry):
        s = lax.rem(me + off, n)

        @pl.when(holder == seat)
        def _():
            slice_relay(s).wait_send()

        return carry

    lax.fori_loop(1, n, drain_slices, 0)
    for i, ref in enumerate((in_gate, conv_input)):
        rim_copy(i, ref).wait_send()
    for q in range(deep):
        gated_over(q).wait_send()
        if q > 0:
            gated_along(q).wait_send()
    mid_sibling().wait_send()
    back_rim.wait_send()
    for q in range(per):
        mid_other(q).wait_send()
        mid_relay(q).wait_send()
        for owner in (member, other):

            @pl.when(owner * per + q != me)
            def _():
                slice_out(owner * per + q).wait_send()


def fused(
    out_grad,
    routes,
    route_weight,
    rows,
    gate_weight,
    up_weight,
    down_weight,
    conv_input,
    out_gate,
    in_gate,
    taps,
    out_weight,
    groups,
):
    n, slots, width = rows.shape
    tokens = out_grad.shape[0]
    ff = gate_weight.shape[1]
    chans = conv_input.shape[1]
    share, span, deep, per = width // groups, width // n, n // 2, n // groups
    dma = pltpu.SemaphoreType.DMA

    def held(*shape):
        return pltpu.VMEM(shape, BF16)

    def exact(*shape):
        return pltpu.VMEM(shape, F32)

    small = jax.ShapeDtypeStruct((tokens, chans), BF16)
    return pl.pallas_call(
        functools.partial(fused_kernel, n, groups),
        out_shape=(
            jax.ShapeDtypeStruct((width, ff), BF16),
            jax.ShapeDtypeStruct((width, ff), BF16),
            jax.ShapeDtypeStruct((ff, width), BF16),
            jax.ShapeDtypeStruct((tokens, share), BF16),
            jax.ShapeDtypeStruct((span, chans), F32),
            small,
            small,
            small,
        ),
        in_specs=[VMEM_SPEC] * 7 + [ANY_SPEC] * 5,
        out_specs=(VMEM_SPEC,) * 8,
        scratch_shapes=[
            held(n, slots, width),
            held(width, 2 * ff),
            held(ff, width),
            held(width, chans),
            exact(n, slots, 2 * ff),
            exact(n, 1, tokens),
            exact(n, 1, tokens),
            held(n, slots, tokens),
            held(n, slots, share),
            held(n, slots, width),
            held(n, slots, ff),
            held(n, slots, 2 * ff),
            held(n, slots, width),
            held(n, 2, slots, share),
            held(n, 2, slots, share),
            held(n, slots, share),
            held(n, slots, share),
            held(n, slots, share),
            exact(tokens, share),
            held(tokens, width),
            held(2, 16, chans),
            exact(16 + tokens, chans),
            exact(tokens, chans),
            held(n, tokens, chans),
            held(n, tokens, span),
            exact(tokens + 8, chans),
            exact(8, chans),
            dma((5,)),
        ]
        + [dma((n,))] * 8
        + [dma((2, n))] * 2
        + [dma((n,))] * 4
        + [dma((2,))] * 2
        + [dma((deep,))] * 4
        + [dma(())] * 2
        + [dma((per,))] * 4
        + [dma((n,))] * 4
        + [dma(())] * 2,
        compiler_params=pltpu.CompilerParams(collective_id=4, has_side_effects=True),
    )(
        out_grad,
        routes.T,
        route_weight.T,
        conv_input,
        out_gate,
        in_gate,
        taps,
        rows,
        gate_weight,
        up_weight,
        down_weight,
        out_weight,
    )


def fits_fused(tokens, slots, width, sources, groups):
    tidy = slots % 16 == 0 and tokens % 16 == 0 and width % (128 * sources) == 0
    return tidy and groups == 4 and sources % 4 == 0


def on_device(
    out_grad,
    routes,
    route_weight,
    expert_rows,
    gate_weight,
    up_weight,
    down_weight,
    conv_input,
    out_gate,
    in_gate,
    taps,
    out_weight,
):
    groups = lax.axis_size("tp")
    sources = lax.axis_size("sp")
    slots, width = expert_rows.shape[2:]
    assert gate_weight.shape[0] == 1
    if not fits_fused(out_grad.shape[0], slots, width, sources, groups):
        return staged(
            out_grad,
            routes,
            route_weight,
            expert_rows,
            gate_weight,
            up_weight,
            down_weight,
            conv_input,
            out_gate,
            in_gate,
            taps,
            out_weight,
        )
    outs = fused(
        out_grad,
        routes,
        route_weight,
        expert_rows.reshape(sources, slots, width),
        gate_weight[0],
        up_weight[0],
        down_weight[0],
        conv_input,
        out_gate,
        in_gate,
        taps,
        out_weight,
        groups,
    )
    return tuple(out[None] for out in outs[:3]) + tuple(outs[3:])


def staged(
    out_grad,
    routes,
    route_weight,
    expert_rows,
    gate_weight,
    up_weight,
    down_weight,
    conv_input,
    out_gate,
    in_gate,
    taps,
    out_weight,
):
    groups = lax.axis_size("tp")
    member = lax.axis_index("tp")
    sources = lax.axis_size("sp")
    tok_rows, width = out_grad.shape
    top = routes.shape[1]
    local = gate_weight.shape[0]
    assert local == 1
    experts = local * sources
    slots = expert_rows.shape[2]
    share = width // groups
    own_cols = lax.dynamic_slice_in_dim(out_grad, member * share, share, 1)
    names = jnp.arange(experts, dtype=jnp.int32)
    named = routes[:, :, None] == names[None, None, :]
    chosen = jnp.any(named, axis=1)
    weight = jnp.sum(jnp.where(named, route_weight[:, :, None], 0.0), axis=1)
    order = jnp.arange(tok_rows, dtype=jnp.int32)
    earlier = (order[:, None] > order[None, :]).astype(jnp.bfloat16)
    place = jnp.dot(
        earlier, chosen.astype(jnp.bfloat16), preferred_element_type=jnp.float32
    ).astype(jnp.int32)
    place = jnp.where(chosen, place, -1).T
    filled = place[:, None, :] == jnp.arange(slots, dtype=jnp.int32)[None, :, None]
    slot_weight = jnp.sum(jnp.where(filled, weight.T[:, None, :], 0.0), axis=2)
    picker = filled.astype(jnp.bfloat16).reshape(experts * slots, tok_rows)
    outgoing = jnp.dot(picker, own_cols, preferred_element_type=jnp.float32)
    outgoing = (slot_weight.reshape(-1, 1) * outgoing).astype(jnp.bfloat16)
    outgoing = outgoing.reshape(sources, local * slots, share)
    rows = expert_rows.reshape(-1, width)
    wide_gate, wide_up, tall_down = gate_weight[0], up_weight[0], down_weight[0]
    grads, gate, up = spread(outgoing, rows, wide_gate, wide_up, groups)
    grads = grads.reshape(-1, width)
    sig = jax.nn.sigmoid(gate)
    act = (gate * sig * up).astype(jnp.bfloat16)
    act_grad = lax.dot_general(
        grads, tall_down, (((1,), (1,)), ((), ())), preferred_element_type=jnp.float32
    )
    up_part = (act_grad * gate * sig).astype(jnp.bfloat16)
    gate_part = (act_grad * up * sig * (1.0 + gate * (1.0 - sig))).astype(jnp.bfloat16)
    row_part = lax.dot_general(
        gate_part, wide_gate, (((1,), (1,)), ((), ())), preferred_element_type=jnp.float32
    )
    row_part = row_part + lax.dot_general(
        up_part, wide_up, (((1,), (1,)), ((), ())), preferred_element_type=jnp.float32
    )
    row_part = row_part.astype(jnp.bfloat16).reshape(sources, slots, width)
    returned, gate_grad, up_grad, down_grad = collect(
        row_part, rows, grads, act, gate_part, up_part, groups
    )
    returned = returned.reshape(experts * slots, share)
    gate_grad, up_grad, down_grad = gate_grad[None], up_grad[None], down_grad[None]
    picked = lax.dot_general(
        picker, returned, (((0,), (0,)), ((), ())), preferred_element_type=jnp.float32
    )
    mid_grad = (own_cols.astype(jnp.float32) + picked).astype(jnp.bfloat16)
    mid_whole = widen(mid_grad, groups)
    reach = taps.shape[0] - 1
    rims = jnp.stack([in_gate[tok_rows - reach :], conv_input[tok_rows - reach :]])
    prior = passed_along(rims, "sp", 1)
    mixed = in_gate.astype(jnp.float32) * conv_input.astype(jnp.float32)
    prior_mixed = prior[0].astype(jnp.float32) * prior[1].astype(jnp.float32)
    extended = jnp.concatenate([prior_mixed, mixed], axis=0)
    conv = jnp.zeros_like(mixed)
    for tap in range(reach + 1):
        conv = conv + taps[tap][None, :] * extended[reach - tap : reach - tap + tok_rows]
    gated = (out_gate.astype(jnp.float32) * conv).astype(jnp.bfloat16)
    partial_grad = lax.dot_general(
        mid_whole, gated, (((0,), (0,)), ((), ())), preferred_element_type=jnp.float32
    ).astype(jnp.bfloat16)
    out_weight_grad = fold(partial_grad.reshape(sources, width // sources, gated.shape[1]))
    gated_grad = jnp.dot(mid_whole, out_weight, preferred_element_type=jnp.float32)
    out_gate_grad = (gated_grad * conv).astype(jnp.bfloat16)
    conv_grad = gated_grad * out_gate.astype(jnp.float32)
    later = passed_along(conv_grad[:reach], "sp", -1)
    following = jnp.concatenate([conv_grad, later], axis=0)
    mixed_grad = jnp.zeros_like(conv_grad)
    for tap in range(reach + 1):
        mixed_grad = mixed_grad + taps[tap][None, :] * following[tap : tap + tok_rows]
    input_grad = (mixed_grad * in_gate.astype(jnp.float32)).astype(jnp.bfloat16)
    in_gate_grad = (mixed_grad * conv_input.astype(jnp.float32)).astype(jnp.bfloat16)
    return (
        gate_grad,
        up_grad,
        down_grad,
        mid_grad,
        out_weight_grad,
        input_grad,
        out_gate_grad,
        in_gate_grad,
    )


def solution(mesh):
    in_specs = (
        P("sp", None),
        P("sp", None),
        P("sp", None),
        P(None, "sp", None, None),
        P("sp", None, "tp"),
        P("sp", None, "tp"),
        P("sp", "tp", None),
        P("sp", "tp"),
        P("sp", "tp"),
        P("sp", "tp"),
        P(None, "tp"),
        P(None, "tp"),
    )
    out_specs = (
        P("sp", None, "tp"),
        P("sp", None, "tp"),
        P("sp", "tp", None),
        P("sp", "tp"),
        P("sp", "tp"),
        P("sp", "tp"),
        P("sp", "tp"),
        P("sp", "tp"),
    )
    return jax.shard_map(
        on_device, mesh=mesh, in_specs=in_specs, out_specs=out_specs, check_vma=False
    )
```

```python
import functools

import jax
import jax.numpy as jnp
from jax import lax
from jax.experimental import pallas as pl
from jax.experimental.pallas import tpu as pltpu
from jax.sharding import PartitionSpec as P

ANY_SPEC = pl.BlockSpec(memory_space=pl.ANY)
VMEM_SPEC = pl.BlockSpec(memory_space=pltpu.VMEM)


def passed_along(shard, axis, by):
    peers = lax.axis_size(axis)
    pairs = [(i, i + by) for i in range(peers) if 0 <= i + by < peers]
    return lax.ppermute(shard, axis, pairs)


def remote(src, dst, send_sem, recv_sem, **target):
    return pltpu.make_async_remote_copy(
        src_ref=src,
        dst_ref=dst,
        send_sem=send_sem,
        recv_sem=recv_sem,
        device_id=target,
        device_id_type=pl.DeviceIdType.MESH,
    )


def greet(sp_peers, tp_peers):
    barrier = pltpu.get_barrier_semaphore()
    for peer in sp_peers:
        pl.semaphore_signal(
            barrier, inc=1, device_id={"sp": peer}, device_id_type=pl.DeviceIdType.MESH
        )
    for peer in tp_peers:
        pl.semaphore_signal(
            barrier, inc=1, device_id={"tp": peer}, device_id_type=pl.DeviceIdType.MESH
        )
    pl.semaphore_wait(barrier, len(sp_peers) + len(tp_peers))


def tp_places(groups):
    member = lax.axis_index("tp")
    sibling = member + 1 - 2 * lax.rem(member, 2)
    others = [lax.rem(member + 2 * d, groups) for d in range(1, groups // 2)]
    return member, sibling, others


def columns(member, share):
    return pl.ds(pl.multiple_of(member * share, share), share)


def spread_kernel(
    n,
    groups,
    send_ref,
    rows_hbm,
    wg_hbm,
    wu_hbm,
    out_ref,
    gate_ref,
    up_ref,
    rows_ref,
    wg_ref,
    wu_ref,
    load_sem,
    own_sem,
    s_a,
    r_a,
    s_f,
    r_f,
    s_g,
    r_g,
):
    me = lax.axis_index("sp")
    member, sibling, others = tp_places(groups)
    share = send_ref.shape[2]
    greet([lax.rem(me + off, n) for off in range(1, n)], [sibling] + others)

    def across(off):
        dest = lax.rem(me + off, n)
        return remote(
            send_ref.at[dest],
            out_ref.at[me, :, columns(member, share)],
            s_a.at[off],
            r_a.at[off],
            sp=dest,
        )

    def block(off, owner):
        return out_ref.at[lax.rem(me + n - off, n), :, columns(owner, share)]

    def hand(off, d):
        target = sibling if d == 0 else others[d - 1]
        return remote(
            block(off, member), block(off, member), s_f.at[d, off], r_f.at[d, off], tp=target
        )

    def relay(off, d):
        piece = block(off, others[d - 1])
        return remote(piece, piece, s_g.at[d - 1, off], r_g.at[d - 1, off], tp=sibling)

    def hand_on(off):
        for d in range(groups // 2):
            hand(off, d).start()

    def relay_on(off):
        for d in range(1, groups // 2):
            hand(off, d).wait_recv()
            relay(off, d).start()

    own = pltpu.make_async_copy(send_ref.at[me], out_ref.at[me, :, columns(member, share)], own_sem)
    own.start()

    def send_out(off, carry):
        across(off).start()
        return carry

    lax.fori_loop(1, n, send_out, 0)
    loads = [
        pltpu.make_async_copy(wg_hbm, wg_ref, load_sem.at[0]),
        pltpu.make_async_copy(wu_hbm, wu_ref, load_sem.at[1]),
        pltpu.make_async_copy(rows_hbm, rows_ref, load_sem.at[2]),
    ]
    for load in loads:
        load.start()
    own.wait()
    hand_on(0)
    tall = rows_ref.shape[0]
    inside = (tall // n) % 16 == 0
    pieces = n if inside else 4
    size = tall // pieces

    def project(piece):
        at = pl.ds(pl.multiple_of(piece * size, size), size)
        rows = rows_ref[at, :]
        gate_ref[at, :] = jnp.dot(rows, wg_ref[...], preferred_element_type=jnp.float32)
        up_ref[at, :] = jnp.dot(rows, wu_ref[...], preferred_element_type=jnp.float32)

    def project_step(piece, carry):
        project(piece)
        return carry

    for load in loads:
        load.wait()
    if inside:
        project(n - 1)
    else:
        lax.fori_loop(0, pieces, project_step, 0)

    def step(off, carry):
        across(off).wait_recv()
        hand_on(off)
        relay_on(off - 1)
        if inside:
            project(off - 1)
        return carry

    lax.fori_loop(1, n, step, 0)
    relay_on(n - 1)

    def finish(off, carry):
        hand(off, 0).wait_recv()
        for d in range(groups // 2):
            hand(off, d).wait_send()
        for d in range(1, groups // 2):
            relay(off, d).wait()
        return carry

    lax.fori_loop(0, n, finish, 0)

    def drain(off, carry):
        across(off).wait_send()
        return carry

    lax.fori_loop(1, n, drain, 0)


def spread(blocks, rows, gate_weight, up_weight, groups):
    n, depth, share = blocks.shape
    hidden = jax.ShapeDtypeStruct((rows.shape[0], gate_weight.shape[1]), jnp.float32)
    dma = pltpu.SemaphoreType.DMA
    return pl.pallas_call(
        functools.partial(spread_kernel, n, groups),
        out_shape=(
            jax.ShapeDtypeStruct((n, depth, share * groups), blocks.dtype),
            hidden,
            hidden,
        ),
        in_specs=[VMEM_SPEC, ANY_SPEC, ANY_SPEC, ANY_SPEC],
        out_specs=(VMEM_SPEC, VMEM_SPEC, VMEM_SPEC),
        scratch_shapes=[
            pltpu.VMEM(rows.shape, rows.dtype),
            pltpu.VMEM(gate_weight.shape, gate_weight.dtype),
            pltpu.VMEM(up_weight.shape, up_weight.dtype),
            dma((3,)),
            dma(()),
            dma((n,)),
            dma((n,)),
            dma((groups // 2, n)),
            dma((groups // 2, n)),
            dma((groups // 2 - 1, n)),
            dma((groups // 2 - 1, n)),
        ],
        compiler_params=pltpu.CompilerParams(collective_id=0, has_side_effects=True),
    )(blocks, rows, gate_weight, up_weight)


def collect_kernel(
    n,
    groups,
    part_ref,
    rows_hbm,
    grads_hbm,
    act_hbm,
    gate_hbm,
    up_hbm,
    out_ref,
    gate_out,
    up_out,
    down_out,
    near,
    pair,
    far,
    final,
    rows_ref,
    grads_ref,
    act_ref,
    gate_ref,
    up_ref,
    load_sem,
    s_n,
    r_n,
    s_f,
    r_f,
    s_a,
    r_a,
):
    me = lax.axis_index("sp")
    member, sibling, others = tp_places(groups)
    half = groups // 2
    share = out_ref.shape[2]
    seat, row = lax.rem(member, 2), lax.div(member, 2)
    greet([lax.rem(me + off, n) for off in range(1, n)], [sibling] + others)

    def home(off):
        return lax.rem(me + off, n)

    def to_sibling(off, h):
        return remote(
            part_ref.at[home(off), :, columns(2 * h + 1 - seat, share)],
            near.at[home(off), h],
            s_n.at[h, off],
            r_n.at[h, off],
            tp=sibling,
        )

    def to_other(off, d):
        h = lax.rem(row + d, half)
        return remote(
            pair.at[home(off), h],
            far.at[d - 1, home(off)],
            s_f.at[d - 1, off],
            r_f.at[d - 1, off],
            tp=others[d - 1],
        )

    def to_home(off):
        return remote(
            final.at[home(off)], out_ref.at[me], s_a.at[off], r_a.at[off], sp=home(off)
        )

    def open_step(i, carry):
        off = lax.rem(i + 1, n)
        for h in range(half):
            to_sibling(off, h).start()
        return carry

    lax.fori_loop(0, n, open_step, 0)
    sources = (act_hbm, gate_hbm, up_hbm, rows_hbm, grads_hbm)
    held = (act_ref, gate_ref, up_ref, rows_ref, grads_ref)
    loads = [pltpu.make_async_copy(a, b, load_sem.at[i]) for i, (a, b) in enumerate(zip(sources, held))]
    for load in loads:
        load.start()
    width = rows_ref.shape[1]
    inside = width % (128 * n) == 0
    pieces = n if inside else 8
    size = width // pieces

    def across_rows(a, b):
        total = lax.dot_general(a, b, (((0,), (0,)), ((), ())), preferred_element_type=jnp.float32)
        return total.astype(jnp.bfloat16)

    def weigh(piece):
        at = columns(piece, size)
        rows = rows_ref[:, at]
        gate_out[at, :] = across_rows(rows, gate_ref[...])
        up_out[at, :] = across_rows(rows, up_ref[...])
        down_out[:, at] = across_rows(act_ref[...], grads_ref[:, at])

    def weigh_step(piece, carry):
        weigh(piece)
        return carry

    def pair_step(i, carry):
        off = lax.rem(i + 1, n)
        for h in range(half):
            to_sibling(off, h).wait_recv()
            mine = part_ref[home(off), :, columns(2 * h + seat, share)].astype(jnp.float32)
            total = mine + near[home(off), h].astype(jnp.float32)
            pair[home(off), h] = total.astype(jnp.bfloat16)
        for d in range(1, half):
            to_other(off, d).start()
        return carry

    lax.fori_loop(0, n, pair_step, 0)

    for load in loads:
        load.wait()
    if inside:
        weigh(n - 1)
    else:
        lax.fori_loop(0, pieces, weigh_step, 0)

    def summed(off):
        total = pair[home(off), row].astype(jnp.float32)
        for d in range(1, half):
            to_other(off, d).wait_recv()
            total = total + far[d - 1, home(off)].astype(jnp.float32)
        return total.astype(jnp.bfloat16)

    def home_step(off, carry):
        final[home(off)] = summed(off)
        to_home(off).start()
        if inside:
            weigh(off - 1)
        return carry

    lax.fori_loop(1, n, home_step, 0)
    out_ref[me] = summed(0)

    def drain(off, carry):
        for h in range(half):
            to_sibling(off, h).wait_send()
        for d in range(1, half):
            to_other(off, d).wait_send()
        return carry

    lax.fori_loop(0, n, drain, 0)

    def arrive(off, carry):
        to_home(off).wait()
        return carry

    lax.fori_loop(1, n, arrive, 0)


def collect(parts, rows, grads, act, gate_part, up_part, groups):
    n, depth, width = parts.shape
    ff = act.shape[1]
    share, half = width // groups, groups // 2
    dma = pltpu.SemaphoreType.DMA
    return pl.pallas_call(
        functools.partial(collect_kernel, n, groups),
        out_shape=(
            jax.ShapeDtypeStruct((n, depth, share), parts.dtype),
            jax.ShapeDtypeStruct((width, ff), parts.dtype),
            jax.ShapeDtypeStruct((width, ff), parts.dtype),
            jax.ShapeDtypeStruct((ff, width), parts.dtype),
        ),
        in_specs=[VMEM_SPEC] + [ANY_SPEC] * 5,
        out_specs=(VMEM_SPEC,) * 4,
        scratch_shapes=[
            pltpu.VMEM((n, half, depth, share), parts.dtype),
            pltpu.VMEM((n, half, depth, share), parts.dtype),
            pltpu.VMEM((half - 1, n, depth, share), parts.dtype),
            pltpu.VMEM((n, depth, share), parts.dtype),
            pltpu.VMEM(rows.shape, rows.dtype),
            pltpu.VMEM(grads.shape, grads.dtype),
            pltpu.VMEM(act.shape, act.dtype),
            pltpu.VMEM(act.shape, act.dtype),
            pltpu.VMEM(act.shape, act.dtype),
            dma((5,)),
            dma((half, n)),
            dma((half, n)),
            dma((half - 1, n)),
            dma((half - 1, n)),
            dma((n,)),
            dma((n,)),
        ],
        compiler_params=pltpu.CompilerParams(collective_id=1, has_side_effects=True),
    )(parts, rows, grads, act, gate_part, up_part)


def widen_kernel(groups, chunks, own_ref, out_ref, own_sem, s_f, r_f, s_g, r_g):
    member, sibling, others = tp_places(groups)
    rows, share = own_ref.shape
    size = rows // chunks
    greet([], [sibling] + others)

    def place(c, owner):
        return out_ref.at[pl.ds(c * size, size), columns(owner, share)]

    def hand(c, d):
        target = sibling if d == 0 else others[d - 1]
        return remote(
            own_ref.at[pl.ds(c * size, size)],
            place(c, member),
            s_f.at[d, c],
            r_f.at[d, c],
            tp=target,
        )

    def relay(c, d):
        piece = place(c, others[d - 1])
        return remote(piece, piece, s_g.at[d - 1, c], r_g.at[d - 1, c], tp=sibling)

    for c in range(chunks):
        for d in range(1, groups // 2):
            hand(c, d).start()
    for c in range(chunks):
        hand(c, 0).start()
    own = pltpu.make_async_copy(own_ref, out_ref.at[:, columns(member, share)], own_sem)
    own.start()
    for c in range(chunks):
        for d in range(1, groups // 2):
            hand(c, d).wait_recv()
            relay(c, d).start()
    own.wait()
    for c in range(chunks):
        hand(c, 0).wait_recv()
        for d in range(groups // 2):
            hand(c, d).wait_send()
        for d in range(1, groups // 2):
            relay(c, d).wait()


def widen(own, groups):
    rows, share = own.shape
    chunks = 4 if rows % 64 == 0 else 1
    dma = pltpu.SemaphoreType.DMA
    return pl.pallas_call(
        functools.partial(widen_kernel, groups, chunks),
        out_shape=jax.ShapeDtypeStruct((rows, share * groups), own.dtype),
        in_specs=[VMEM_SPEC],
        out_specs=VMEM_SPEC,
        scratch_shapes=[
            dma(()),
            dma((groups // 2, chunks)),
            dma((groups // 2, chunks)),
            dma((groups // 2 - 1, chunks)),
            dma((groups // 2 - 1, chunks)),
        ],
        compiler_params=pltpu.CompilerParams(collective_id=2, has_side_effects=True),
    )(own)


def fold_kernel(n, part_ref, out_ref, near, pair, far, s_n, r_n, s_f, r_f):
    me = lax.axis_index("sp")
    seat, row = lax.rem(me, 2), lax.div(me, 2)
    partner = me + 1 - 2 * seat
    half = n // 2
    greet([partner] + [lax.rem(me + 2 * d, n) for d in range(1, half)], [])

    def spot(d):
        return lax.rem(row + d, half)

    def to_partner(d):
        return remote(
            part_ref.at[2 * spot(d) + 1 - seat], near.at[d], s_n.at[d], r_n.at[d], sp=partner
        )

    def to_owner(d):
        return remote(
            pair.at[d], far.at[d], s_f.at[d], r_f.at[d], sp=lax.rem(me + 2 * d, n)
        )

    def open_step(i, carry):
        to_partner(lax.rem(i + 1, half)).start()
        return carry

    lax.fori_loop(0, half, open_step, 0)

    def paired(d):
        to_partner(d).wait_recv()
        mine = part_ref[2 * spot(d) + seat].astype(jnp.float32)
        return mine + near[d].astype(jnp.float32)

    def pair_step(d, carry):
        pair[d] = paired(d).astype(jnp.bfloat16)
        to_owner(d).start()
        return carry

    lax.fori_loop(1, half, pair_step, 0)
    out_ref[...] = paired(0)

    def add_step(d, carry):
        to_owner(d).wait_recv()
        out_ref[...] += far[d].astype(jnp.float32)
        return carry

    lax.fori_loop(1, half, add_step, 0)

    def drain(d, carry):
        to_partner(d).wait_send()
        return carry

    lax.fori_loop(0, half, drain, 0)

    def drain_owner(d, carry):
        to_owner(d).wait_send()
        return carry

    lax.fori_loop(1, half, drain_owner, 0)


def fold(parts):
    n, rows, cols = parts.shape
    half = n // 2
    dma = pltpu.SemaphoreType.DMA
    return pl.pallas_call(
        functools.partial(fold_kernel, n),
        out_shape=jax.ShapeDtypeStruct((rows, cols), jnp.float32),
        in_specs=[VMEM_SPEC],
        out_specs=VMEM_SPEC,
        scratch_shapes=[
            pltpu.VMEM((half, rows, cols), parts.dtype),
            pltpu.VMEM((half, rows, cols), parts.dtype),
            pltpu.VMEM((half, rows, cols), parts.dtype),
            dma((half,)),
            dma((half,)),
            dma((half,)),
            dma((half,)),
        ],
        compiler_params=pltpu.CompilerParams(collective_id=3, has_side_effects=True),
    )(parts)


HBM_SPEC = pl.BlockSpec(memory_space=pltpu.HBM)
BF16, F32 = jnp.bfloat16, jnp.float32


def dot_nn(a, b):
    return jnp.dot(a, b, preferred_element_type=F32)


def dot_nt(a, b):
    return lax.dot_general(a, b, (((1,), (1,)), ((), ())), preferred_element_type=F32)


def dot_tn(a, b):
    return lax.dot_general(a, b, (((0,), (0,)), ((), ())), preferred_element_type=F32)


def fused_kernel(
    n,
    groups,
    out_grad_hbm,
    routes_hbm,
    route_weight_hbm,
    conv_input_hbm,
    out_gate_hbm,
    in_gate_hbm,
    taps_hbm,
    rows_hbm,
    wg_hbm,
    wu_hbm,
    dn_hbm,
    ow_hbm,
    gate_out,
    up_out,
    down_out,
    mid_out,
    weight_out,
    input_out,
    out_gate_out,
    in_gate_out,
    out_grad,
    routes,
    route_weight,
    conv_input,
    out_gate,
    in_gate,
    taps,
    rows,
    wgu,
    dn,
    ow,
    hidden,
    place,
    weight,
    picker,
    send,
    grads,
    act,
    parts,
    row_part,
    near,
    pair,
    far,
    final,
    back,
    total,
    wide,
    rim,
    mixed,
    conv,
    gated,
    slices,
    follow,
    later,
    load_sem,
    s_a,
    r_a,
    s_x,
    r_x,
    s_b,
    r_b,
    s_g,
    r_g,
    s_n,
    r_n,
    s_f,
    r_f,
    s_h,
    r_h,
    s_rim,
    r_rim,
    s_d,
    r_d,
    s_p,
    r_p,
    s_m,
    r_m,
    s_mx,
    r_mx,
    s_mr,
    r_mr,
    s_v,
    r_v,
    s_w,
    r_w,
    s_l,
    r_l,
):
    me = lax.axis_index("sp")
    member = lax.axis_index("tp")
    seat = lax.rem(member, 2)
    line = lax.div(member, 2)
    sibling = member + 1 - 2 * seat
    other = lax.rem(member + 2, groups)
    tokens, width = out_grad.shape
    slots = rows.shape[1]
    ff = dn.shape[0]
    share = width // groups
    deep = n // 2
    per = n // groups
    span = width // n

    barrier = pltpu.get_barrier_semaphore()

    def call(off, carry):
        pl.semaphore_signal(
            barrier,
            inc=1,
            device_id={"sp": lax.rem(me + off, n)},
            device_id_type=pl.DeviceIdType.MESH,
        )
        return carry

    lax.fori_loop(1, n, call, 0)
    for peer in (sibling, other):
        pl.semaphore_signal(
            barrier, inc=1, device_id={"tp": peer}, device_id_type=pl.DeviceIdType.MESH
        )
    early = [
        pltpu.make_async_copy(routes_hbm, routes, load_sem.at[5]),
        pltpu.make_async_copy(route_weight_hbm, route_weight, load_sem.at[6]),
        pltpu.make_async_copy(out_grad_hbm, out_grad, load_sem.at[7]),
        pltpu.make_async_copy(in_gate_hbm, in_gate, load_sem.at[8]),
        pltpu.make_async_copy(conv_input_hbm, conv_input, load_sem.at[9]),
        pltpu.make_async_copy(out_gate_hbm, out_gate, load_sem.at[10]),
        pltpu.make_async_copy(taps_hbm, taps, load_sem.at[11]),
    ]
    loads = [
        pltpu.make_async_copy(wg_hbm, wgu.at[:, pl.ds(0, ff)], load_sem.at[0]),
        pltpu.make_async_copy(wu_hbm, wgu.at[:, pl.ds(ff, ff)], load_sem.at[1]),
        pltpu.make_async_copy(rows_hbm, rows, load_sem.at[2]),
        pltpu.make_async_copy(dn_hbm, dn, load_sem.at[3]),
        pltpu.make_async_copy(ow_hbm, ow, load_sem.at[4]),
    ]
    for load in early + loads:
        load.start()

    def shift(k, way):
        q = lax.div(k, 2)
        step = lax.div(q + 1, 2) * (2 * lax.rem(q, 2) - 1) * way
        deeper = lax.rem(lax.div(me, 2) + step + deep, deep)
        side = lax.rem(lax.rem(me, 2) + lax.rem(k, 2), 2)
        return 2 * deeper + side

    def dest(k):
        return shift(k, 1)

    def source(k):
        return shift(k, -1)

    def slice_at(j):
        return pl.ds(pl.multiple_of(j * span, span), span)

    def across(k):
        return remote(
            send.at[dest(k)],
            grads.at[me, :, columns(member, share)],
            s_a.at[k],
            r_a.at[k],
            sp=dest(k),
        )

    def hand(k):
        piece = grads.at[source(k), :, columns(member, share)]
        return remote(piece, piece, s_b.at[k], r_b.at[k], tp=sibling)

    def cross(k):
        piece = grads.at[source(k), :, columns(member, share)]
        return remote(piece, piece, s_x.at[k], r_x.at[k], tp=other)

    def relay(k):
        piece = grads.at[source(k), :, columns(other, share)]
        return remote(piece, piece, s_g.at[k], r_g.at[k], tp=sibling)

    def to_sibling(k, h):
        return remote(
            row_part.at[source(k), :, columns(2 * h + 1 - seat, share)],
            near.at[source(k), h],
            s_n.at[h, k],
            r_n.at[h, k],
            tp=sibling,
        )

    def to_other(k):
        return remote(
            pair.at[source(k), 1 - line], far.at[source(k)], s_f.at[k], r_f.at[k], tp=other
        )

    def to_home(k):
        return remote(final.at[source(k)], back.at[me], s_h.at[k], r_h.at[k], sp=source(k))

    def rim_copy(i, ref):
        return remote(
            ref.at[pl.ds(tokens - 16, 16)],
            rim.at[i],
            s_rim.at[i],
            r_rim.at[i],
            sp=lax.rem(me + 1, n),
        )

    def gated_along(q):
        return remote(gated.at[me], gated.at[me], s_d.at[q], r_d.at[q], sp=dest(2 * q))

    def gated_over(q):
        piece = gated.at[source(2 * q)]
        return remote(piece, piece, s_p.at[q], r_p.at[q], sp=dest(1))

    for load in early[:2]:
        load.wait()
    names = lax.broadcasted_iota(jnp.int32, (n, tokens), 0)
    chosen = jnp.zeros((n, tokens), jnp.bool_)
    weights = jnp.zeros((n, tokens), F32)
    for choice in range(routes.shape[0]):
        named = names == routes[choice : choice + 1, :]
        chosen = jnp.logical_or(chosen, named)
        weights = weights + jnp.where(named, route_weight[choice : choice + 1, :], 0.0)
    first = lax.broadcasted_iota(jnp.int32, (tokens, tokens), 0)
    second = lax.broadcasted_iota(jnp.int32, (tokens, tokens), 1)
    earlier = jnp.where(first < second, 1.0, 0.0).astype(BF16)
    marks = jnp.where(chosen, 1.0, 0.0)
    places = jnp.where(chosen, dot_nn(marks.astype(BF16), earlier), -1.0)
    for e in range(n):
        place[e] = places[e : e + 1, :]
        weight[e] = weights[e : e + 1, :]
    seats = lax.broadcasted_iota(jnp.int32, (slots, tokens), 0).astype(F32)

    def pick(e):
        filled = place[e] == seats
        found = jnp.where(filled, 1.0, 0.0).astype(BF16)
        picker[e] = found
        held = jnp.sum(jnp.where(filled, weight[e], 0.0), axis=1, keepdims=True)
        return found, held

    for load in early[2:]:
        load.wait()
    pl.semaphore_wait(barrier, n + 1)
    for i, ref in enumerate((in_gate, conv_input)):
        rim_copy(i, ref).start()

    def build(k, carry):
        e = dest(k)
        found, held = pick(e)
        own = dot_nn(found, out_grad[:, columns(member, share)])
        send[e] = (held * own).astype(BF16)
        across(k).start()
        return carry

    lax.fori_loop(1, n, build, 0)
    found, held = pick(me)
    for g in range(groups):
        at = pl.ds(g * share, share)
        grads[me, :, at] = (held * dot_nn(found, out_grad[:, at])).astype(BF16)
    for load in loads[:3]:
        load.wait()
    couples = 2

    def project(c, carry):
        at = pl.ds(c * couples, couples)
        rows_c = rows[at].reshape(couples * slots, width)
        hidden[at] = dot_nn(rows_c, wgu[...]).reshape(couples, slots, 2 * ff)
        return carry

    lax.fori_loop(0, n // couples, project, 0)

    for i, ref in enumerate((in_gate, conv_input)):
        rim_copy(i, ref).wait_recv()
    prior = rim[0].astype(F32) * rim[1].astype(F32)
    mixed[0:16] = jnp.where(me == 0, 0.0, prior)
    mixed[pl.ds(16, tokens)] = in_gate[...].astype(F32) * conv_input[...].astype(F32)
    reach = taps.shape[0]
    conv_sum = taps[0:1, :] * mixed[pl.ds(16, tokens)]
    for tap in range(1, reach):
        conv_sum = conv_sum + taps[tap : tap + 1, :] * mixed[pl.ds(16 - tap, tokens)]
    conv[...] = conv_sum
    gated[me] = (out_gate[...].astype(F32) * conv_sum).astype(BF16)
    for q in range(1, deep):
        gated_along(q).start()
    gated_over(0).start()
    loads[3].wait()
    loads[4].wait()

    def arrive(k):
        across(k).wait_recv()
        cross(k).start()
        hand(k).start()

    def pass_on(k):
        cross(k).wait_recv()
        relay(k).start()

    def backward(k):
        @pl.when(k > 0)
        def _():
            hand(k).wait_recv()
            relay(k).wait_recv()

        s = source(k)
        gate = hidden[s, :, 0:ff]
        up = hidden[s, :, ff : 2 * ff]
        sig = jax.nn.sigmoid(gate)
        act[s] = (gate * sig * up).astype(BF16)
        act_grad = dot_nt(grads[s], dn[...])
        parts[s, :, 0:ff] = (act_grad * up * sig * (1.0 + gate * (1.0 - sig))).astype(BF16)
        parts[s, :, ff : 2 * ff] = (act_grad * gate * sig).astype(BF16)
        both = parts[s]
        for g in range(groups):
            at = pl.ds(g * share, share)
            row_part[s, :, at] = dot_nt(both, wgu[at, :]).astype(BF16)
        for h in range(2):
            to_sibling(k, h).start()

    def pair_up(k):
        s = source(k)
        for h in range(2):
            to_sibling(k, h).wait_recv()
            mine = row_part[s, :, columns(2 * h + seat, share)].astype(F32)
            pair[s, h] = (mine + near[s, h].astype(F32)).astype(BF16)
        to_other(k).start()

    def finish(k):
        s = source(k)
        to_other(k).wait_recv()
        final[s] = (pair[s, line].astype(F32) + far[s].astype(F32)).astype(BF16)

        @pl.when(k > 0)
        def _():
            to_home(k).start()

    def within(k, low, act_on):
        @pl.when(jnp.logical_and(k >= low, k < n))
        def _():
            act_on(k)

    def step(j, carry):
        within(j + 1, 1, arrive)
        within(j, 1, pass_on)
        within(j - 1, 0, backward)
        within(j - 2, 0, pair_up)
        within(j - 3, 0, finish)
        return carry

    lax.fori_loop(0, n + 3, step, 0)

    for q in range(1, deep):
        gated_along(q).wait_recv()
        gated_over(q).start()

    total[...] = out_grad[:, columns(member, share)].astype(F32) + dot_tn(picker[me], final[me])

    def gather_home(k, carry):
        e = dest(k)
        to_home(k).wait_recv()
        total[...] += dot_tn(picker[e], back[e])
        return carry

    lax.fori_loop(1, n, gather_home, 0)
    mid = total[...].astype(BF16)
    mid_out[...] = mid
    wide[:, columns(member, share)] = mid

    def mid_sibling():
        piece = wide.at[:, columns(member, share)]
        return remote(piece, piece, s_m, r_m, tp=sibling)

    def mid_other(q):
        piece = wide.at[:, slice_at(member * per + q)]
        return remote(piece, piece, s_mx.at[q], r_mx.at[q], tp=other)

    def mid_relay(q):
        piece = wide.at[:, slice_at(other * per + q)]
        return remote(piece, piece, s_mr.at[q], r_mr.at[q], tp=sibling)

    def slice_out(j):
        return remote(wide.at[:, slice_at(j)], slices.at[me], s_v.at[j], r_v.at[me], sp=j)

    def slice_in(s):
        return remote(wide.at[:, slice_at(me)], slices.at[s], s_v.at[s], r_v.at[s], sp=s)

    def slice_relay(s):
        piece = slices.at[s]
        return remote(piece, piece, s_w.at[s], r_w.at[s], tp=sibling)

    def send_slice(j):
        @pl.when(j != me)
        def _():
            slice_out(j).start()

    for q in range(per):
        mid_other(q).start()
    mid_sibling().start()
    for q in range(per):
        send_slice(member * per + q)

    chunk = 128 if width % 256 else 256
    chunks = width // chunk

    def weigh(piece, carry):
        at = columns(piece, chunk)
        tall = n * slots
        grown = dot_tn(rows[:, :, at].reshape(tall, chunk), parts[...].reshape(tall, 2 * ff))
        gate_out[at, :] = grown[:, 0:ff].astype(BF16)
        up_out[at, :] = grown[:, ff : 2 * ff].astype(BF16)
        down_out[:, at] = dot_tn(
            act[...].reshape(tall, ff), grads[:, :, at].reshape(tall, chunk)
        ).astype(BF16)
        return carry

    lax.fori_loop(0, chunks // 2, weigh, 0)
    for q in range(per):
        mid_other(q).wait_recv()
        mid_relay(q).start()
        send_slice(other * per + q)
    lax.fori_loop(chunks // 2, chunks, weigh, 0)
    mid_sibling().wait_recv()
    for q in range(per):
        mid_relay(q).wait_recv()
    gated_grad = dot_nn(wide[...], ow[...])
    conv_grad = gated_grad * out_gate[...].astype(F32)
    follow[pl.ds(0, tokens)] = conv_grad

    back_rim = remote(
        follow.at[pl.ds(0, 8)], later, s_l, r_l, sp=lax.rem(me + n - 1, n)
    )
    back_rim.start()
    out_gate_out[...] = (gated_grad * conv[...]).astype(BF16)
    for q in range(deep):
        gated_over(q).wait_recv()
    weight_out[...] = dot_tn(wide[:, slice_at(me)], gated[me])
    holder = lax.rem(lax.div(me, per), 2)

    def meet(off, carry):
        s = lax.rem(me + off, n)

        @pl.when(holder == seat)
        def _():
            slice_in(s).wait_recv()
            slice_relay(s).start()

        @pl.when(holder != seat)
        def _():
            slice_relay(s).wait_recv()

        weight_out[...] += dot_tn(slices[s], gated[s])
        return carry

    lax.fori_loop(1, n, meet, 0)
    back_rim.wait_recv()
    follow[pl.ds(tokens, 8)] = jnp.where(me == n - 1, 0.0, later[...])
    mixed_grad = taps[0:1, :] * follow[pl.ds(0, tokens)]
    for tap in range(1, reach):
        mixed_grad = mixed_grad + taps[tap : tap + 1, :] * follow[pl.ds(tap, tokens)]
    input_out[...] = (mixed_grad * in_gate[...].astype(F32)).astype(BF16)
    in_gate_out[...] = (mixed_grad * conv_input[...].astype(F32)).astype(BF16)

    def drain(k, carry):
        @pl.when(k > 0)
        def _():
            across(k).wait_send()
            hand(k).wait_send()
            cross(k).wait_send()
            relay(k).wait_send()
            to_home(k).wait_send()

        for h in range(2):
            to_sibling(k, h).wait_send()
        to_other(k).wait_send()
        return carry

    lax.fori_loop(0, n, drain, 0)

    def drain_slices(off, carry):
        s = lax.rem(me + off, n)

        @pl.when(holder == seat)
        def _():
            slice_relay(s).wait_send()

        return carry

    lax.fori_loop(1, n, drain_slices, 0)
    for i, ref in enumerate((in_gate, conv_input)):
        rim_copy(i, ref).wait_send()
    for q in range(deep):
        gated_over(q).wait_send()
        if q > 0:
            gated_along(q).wait_send()
    mid_sibling().wait_send()
    back_rim.wait_send()
    for q in range(per):
        mid_other(q).wait_send()
        mid_relay(q).wait_send()
        for owner in (member, other):

            @pl.when(owner * per + q != me)
            def _():
                slice_out(owner * per + q).wait_send()


def settle_kernel(count, *refs):
    sources, targets, sem = refs[:count], refs[count : 2 * count], refs[2 * count]
    moves = [pltpu.make_async_copy(a, b, sem.at[i]) for i, (a, b) in enumerate(zip(sources, targets))]
    for move in moves:
        move.start()
    for move in moves:
        move.wait()


def settle(arrays):
    count = len(arrays)
    return pl.pallas_call(
        functools.partial(settle_kernel, count),
        out_shape=tuple(jax.ShapeDtypeStruct(a.shape, a.dtype) for a in arrays),
        in_specs=[ANY_SPEC] * count,
        out_specs=(HBM_SPEC,) * count,
        scratch_shapes=[pltpu.SemaphoreType.DMA((count,))],
        compiler_params=pltpu.CompilerParams(vmem_limit_bytes=2**20),
    )(*arrays)


def fused(
    out_grad,
    routes,
    route_weight,
    rows,
    gate_weight,
    up_weight,
    down_weight,
    conv_input,
    out_gate,
    in_gate,
    taps,
    out_weight,
    groups,
):
    n, slots, width = rows.shape
    tokens = out_grad.shape[0]
    ff = gate_weight.shape[1]
    chans = conv_input.shape[1]
    share, span, deep, per = width // groups, width // n, n // 2, n // groups
    dma = pltpu.SemaphoreType.DMA

    def held(*shape):
        return pltpu.VMEM(shape, BF16)

    def exact(*shape):
        return pltpu.VMEM(shape, F32)

    operands = (
        out_grad,
        routes.T,
        route_weight.T,
        conv_input,
        out_gate,
        in_gate,
        taps,
        rows,
        gate_weight,
        up_weight,
        down_weight,
        out_weight,
    )
    small = held(tokens, chans)
    return pl.pallas_call(
        functools.partial(fused_kernel, n, groups),
        out_shape=(
            held(width, ff),
            held(width, ff),
            held(ff, width),
            held(tokens, share),
            exact(span, chans),
            small,
            small,
            small,
        ),
        in_specs=[HBM_SPEC] * 12,
        out_specs=(VMEM_SPEC,) * 8,
        scratch_shapes=[
            held(tokens, width),
            pltpu.VMEM(routes.T.shape, routes.dtype),
            exact(*route_weight.T.shape),
            held(tokens, chans),
            held(tokens, chans),
            held(tokens, chans),
            exact(*taps.shape),
            held(n, slots, width),
            held(width, 2 * ff),
            held(ff, width),
            held(width, chans),
            exact(n, slots, 2 * ff),
            exact(n, 1, tokens),
            exact(n, 1, tokens),
            held(n, slots, tokens),
            held(n, slots, share),
            held(n, slots, width),
            held(n, slots, ff),
            held(n, slots, 2 * ff),
            held(n, slots, width),
            held(n, 2, slots, share),
            held(n, 2, slots, share),
            held(n, slots, share),
            held(n, slots, share),
            held(n, slots, share),
            exact(tokens, share),
            held(tokens, width),
            held(2, 16, chans),
            exact(16 + tokens, chans),
            exact(tokens, chans),
            held(n, tokens, chans),
            held(n, tokens, span),
            exact(tokens + 8, chans),
            exact(8, chans),
            dma((12,)),
        ]
        + [dma((n,))] * 8
        + [dma((2, n))] * 2
        + [dma((n,))] * 4
        + [dma((2,))] * 2
        + [dma((deep,))] * 4
        + [dma(())] * 2
        + [dma((per,))] * 4
        + [dma((n,))] * 4
        + [dma(())] * 2,
        compiler_params=pltpu.CompilerParams(
            collective_id=4, has_side_effects=True, vmem_limit_bytes=40 * 2**20
        ),
    )(*(pltpu.with_memory_space_constraint(a, pltpu.HBM) for a in operands))


def fits_fused(tokens, slots, width, sources, groups):
    tidy = slots % 16 == 0 and tokens % 16 == 0 and width % (128 * sources) == 0
    return tidy and groups == 4 and sources % 4 == 0


def on_device(
    out_grad,
    routes,
    route_weight,
    expert_rows,
    gate_weight,
    up_weight,
    down_weight,
    conv_input,
    out_gate,
    in_gate,
    taps,
    out_weight,
):
    groups = lax.axis_size("tp")
    sources = lax.axis_size("sp")
    slots, width = expert_rows.shape[2:]
    assert gate_weight.shape[0] == 1
    if not fits_fused(out_grad.shape[0], slots, width, sources, groups):
        return staged(
            out_grad,
            routes,
            route_weight,
            expert_rows,
            gate_weight,
            up_weight,
            down_weight,
            conv_input,
            out_gate,
            in_gate,
            taps,
            out_weight,
        )
    outs = fused(
        out_grad,
        routes,
        route_weight,
        expert_rows.reshape(sources, slots, width),
        gate_weight[0],
        up_weight[0],
        down_weight[0],
        conv_input,
        out_gate,
        in_gate,
        taps,
        out_weight,
        groups,
    )
    outs = settle(outs)
    return tuple(out[None] for out in outs[:3]) + tuple(outs[3:])


def staged(
    out_grad,
    routes,
    route_weight,
    expert_rows,
    gate_weight,
    up_weight,
    down_weight,
    conv_input,
    out_gate,
    in_gate,
    taps,
    out_weight,
):
    groups = lax.axis_size("tp")
    member = lax.axis_index("tp")
    sources = lax.axis_size("sp")
    tok_rows, width = out_grad.shape
    top = routes.shape[1]
    local = gate_weight.shape[0]
    assert local == 1
    experts = local * sources
    slots = expert_rows.shape[2]
    share = width // groups
    own_cols = lax.dynamic_slice_in_dim(out_grad, member * share, share, 1)
    names = jnp.arange(experts, dtype=jnp.int32)
    named = routes[:, :, None] == names[None, None, :]
    chosen = jnp.any(named, axis=1)
    weight = jnp.sum(jnp.where(named, route_weight[:, :, None], 0.0), axis=1)
    order = jnp.arange(tok_rows, dtype=jnp.int32)
    earlier = (order[:, None] > order[None, :]).astype(jnp.bfloat16)
    place = jnp.dot(
        earlier, chosen.astype(jnp.bfloat16), preferred_element_type=jnp.float32
    ).astype(jnp.int32)
    place = jnp.where(chosen, place, -1).T
    filled = place[:, None, :] == jnp.arange(slots, dtype=jnp.int32)[None, :, None]
    slot_weight = jnp.sum(jnp.where(filled, weight.T[:, None, :], 0.0), axis=2)
    picker = filled.astype(jnp.bfloat16).reshape(experts * slots, tok_rows)
    outgoing = jnp.dot(picker, own_cols, preferred_element_type=jnp.float32)
    outgoing = (slot_weight.reshape(-1, 1) * outgoing).astype(jnp.bfloat16)
    outgoing = outgoing.reshape(sources, local * slots, share)
    rows = expert_rows.reshape(-1, width)
    wide_gate, wide_up, tall_down = gate_weight[0], up_weight[0], down_weight[0]
    grads, gate, up = spread(outgoing, rows, wide_gate, wide_up, groups)
    grads = grads.reshape(-1, width)
    sig = jax.nn.sigmoid(gate)
    act = (gate * sig * up).astype(jnp.bfloat16)
    act_grad = lax.dot_general(
        grads, tall_down, (((1,), (1,)), ((), ())), preferred_element_type=jnp.float32
    )
    up_part = (act_grad * gate * sig).astype(jnp.bfloat16)
    gate_part = (act_grad * up * sig * (1.0 + gate * (1.0 - sig))).astype(jnp.bfloat16)
    row_part = lax.dot_general(
        gate_part, wide_gate, (((1,), (1,)), ((), ())), preferred_element_type=jnp.float32
    )
    row_part = row_part + lax.dot_general(
        up_part, wide_up, (((1,), (1,)), ((), ())), preferred_element_type=jnp.float32
    )
    row_part = row_part.astype(jnp.bfloat16).reshape(sources, slots, width)
    returned, gate_grad, up_grad, down_grad = collect(
        row_part, rows, grads, act, gate_part, up_part, groups
    )
    returned = returned.reshape(experts * slots, share)
    gate_grad, up_grad, down_grad = gate_grad[None], up_grad[None], down_grad[None]
    picked = lax.dot_general(
        picker, returned, (((0,), (0,)), ((), ())), preferred_element_type=jnp.float32
    )
    mid_grad = (own_cols.astype(jnp.float32) + picked).astype(jnp.bfloat16)
    mid_whole = widen(mid_grad, groups)
    reach = taps.shape[0] - 1
    rims = jnp.stack([in_gate[tok_rows - reach :], conv_input[tok_rows - reach :]])
    prior = passed_along(rims, "sp", 1)
    mixed = in_gate.astype(jnp.float32) * conv_input.astype(jnp.float32)
    prior_mixed = prior[0].astype(jnp.float32) * prior[1].astype(jnp.float32)
    extended = jnp.concatenate([prior_mixed, mixed], axis=0)
    conv = jnp.zeros_like(mixed)
    for tap in range(reach + 1):
        conv = conv + taps[tap][None, :] * extended[reach - tap : reach - tap + tok_rows]
    gated = (out_gate.astype(jnp.float32) * conv).astype(jnp.bfloat16)
    partial_grad = lax.dot_general(
        mid_whole, gated, (((0,), (0,)), ((), ())), preferred_element_type=jnp.float32
    ).astype(jnp.bfloat16)
    out_weight_grad = fold(partial_grad.reshape(sources, width // sources, gated.shape[1]))
    gated_grad = jnp.dot(mid_whole, out_weight, preferred_element_type=jnp.float32)
    out_gate_grad = (gated_grad * conv).astype(jnp.bfloat16)
    conv_grad = gated_grad * out_gate.astype(jnp.float32)
    later = passed_along(conv_grad[:reach], "sp", -1)
    following = jnp.concatenate([conv_grad, later], axis=0)
    mixed_grad = jnp.zeros_like(conv_grad)
    for tap in range(reach + 1):
        mixed_grad = mixed_grad + taps[tap][None, :] * following[tap : tap + tok_rows]
    input_grad = (mixed_grad * in_gate.astype(jnp.float32)).astype(jnp.bfloat16)
    in_gate_grad = (mixed_grad * conv_input.astype(jnp.float32)).astype(jnp.bfloat16)
    return (
        gate_grad,
        up_grad,
        down_grad,
        mid_grad,
        out_weight_grad,
        input_grad,
        out_gate_grad,
        in_gate_grad,
    )


def solution(mesh):
    in_specs = (
        P("sp", None),
        P("sp", None),
        P("sp", None),
        P(None, "sp", None, None),
        P("sp", None, "tp"),
        P("sp", None, "tp"),
        P("sp", "tp", None),
        P("sp", "tp"),
        P("sp", "tp"),
        P("sp", "tp"),
        P(None, "tp"),
        P(None, "tp"),
    )
    out_specs = (
        P("sp", None, "tp"),
        P("sp", None, "tp"),
        P("sp", "tp", None),
        P("sp", "tp"),
        P("sp", "tp"),
        P("sp", "tp"),
        P("sp", "tp"),
        P("sp", "tp"),
    )
    return jax.shard_map(
        on_device, mesh=mesh, in_specs=in_specs, out_specs=out_specs, check_vma=False
    )
```

```python
import functools

import jax
import jax.numpy as jnp
from jax import lax
from jax.experimental import pallas as pl
from jax.experimental.pallas import tpu as pltpu
from jax.sharding import PartitionSpec as P

ANY_SPEC = pl.BlockSpec(memory_space=pl.ANY)
VMEM_SPEC = pl.BlockSpec(memory_space=pltpu.VMEM)


def passed_along(shard, axis, by):
    peers = lax.axis_size(axis)
    pairs = [(i, i + by) for i in range(peers) if 0 <= i + by < peers]
    return lax.ppermute(shard, axis, pairs)


def remote(src, dst, send_sem, recv_sem, **target):
    return pltpu.make_async_remote_copy(
        src_ref=src,
        dst_ref=dst,
        send_sem=send_sem,
        recv_sem=recv_sem,
        device_id=target,
        device_id_type=pl.DeviceIdType.MESH,
    )


def greet(sp_peers, tp_peers):
    barrier = pltpu.get_barrier_semaphore()
    for peer in sp_peers:
        pl.semaphore_signal(
            barrier, inc=1, device_id={"sp": peer}, device_id_type=pl.DeviceIdType.MESH
        )
    for peer in tp_peers:
        pl.semaphore_signal(
            barrier, inc=1, device_id={"tp": peer}, device_id_type=pl.DeviceIdType.MESH
        )
    pl.semaphore_wait(barrier, len(sp_peers) + len(tp_peers))


def tp_places(groups):
    member = lax.axis_index("tp")
    sibling = member + 1 - 2 * lax.rem(member, 2)
    others = [lax.rem(member + 2 * d, groups) for d in range(1, groups // 2)]
    return member, sibling, others


def columns(member, share):
    return pl.ds(pl.multiple_of(member * share, share), share)


def spread_kernel(
    n,
    groups,
    send_ref,
    rows_hbm,
    wg_hbm,
    wu_hbm,
    out_ref,
    gate_ref,
    up_ref,
    rows_ref,
    wg_ref,
    wu_ref,
    load_sem,
    own_sem,
    s_a,
    r_a,
    s_f,
    r_f,
    s_g,
    r_g,
):
    me = lax.axis_index("sp")
    member, sibling, others = tp_places(groups)
    share = send_ref.shape[2]
    greet([lax.rem(me + off, n) for off in range(1, n)], [sibling] + others)

    def across(off):
        dest = lax.rem(me + off, n)
        return remote(
            send_ref.at[dest],
            out_ref.at[me, :, columns(member, share)],
            s_a.at[off],
            r_a.at[off],
            sp=dest,
        )

    def block(off, owner):
        return out_ref.at[lax.rem(me + n - off, n), :, columns(owner, share)]

    def hand(off, d):
        target = sibling if d == 0 else others[d - 1]
        return remote(
            block(off, member), block(off, member), s_f.at[d, off], r_f.at[d, off], tp=target
        )

    def relay(off, d):
        piece = block(off, others[d - 1])
        return remote(piece, piece, s_g.at[d - 1, off], r_g.at[d - 1, off], tp=sibling)

    def hand_on(off):
        for d in range(groups // 2):
            hand(off, d).start()

    def relay_on(off):
        for d in range(1, groups // 2):
            hand(off, d).wait_recv()
            relay(off, d).start()

    own = pltpu.make_async_copy(send_ref.at[me], out_ref.at[me, :, columns(member, share)], own_sem)
    own.start()

    def send_out(off, carry):
        across(off).start()
        return carry

    lax.fori_loop(1, n, send_out, 0)
    loads = [
        pltpu.make_async_copy(wg_hbm, wg_ref, load_sem.at[0]),
        pltpu.make_async_copy(wu_hbm, wu_ref, load_sem.at[1]),
        pltpu.make_async_copy(rows_hbm, rows_ref, load_sem.at[2]),
    ]
    for load in loads:
        load.start()
    own.wait()
    hand_on(0)
    tall = rows_ref.shape[0]
    inside = (tall // n) % 16 == 0
    pieces = n if inside else 4
    size = tall // pieces

    def project(piece):
        at = pl.ds(pl.multiple_of(piece * size, size), size)
        rows = rows_ref[at, :]
        gate_ref[at, :] = jnp.dot(rows, wg_ref[...], preferred_element_type=jnp.float32)
        up_ref[at, :] = jnp.dot(rows, wu_ref[...], preferred_element_type=jnp.float32)

    def project_step(piece, carry):
        project(piece)
        return carry

    for load in loads:
        load.wait()
    if inside:
        project(n - 1)
    else:
        lax.fori_loop(0, pieces, project_step, 0)

    def step(off, carry):
        across(off).wait_recv()
        hand_on(off)
        relay_on(off - 1)
        if inside:
            project(off - 1)
        return carry

    lax.fori_loop(1, n, step, 0)
    relay_on(n - 1)

    def finish(off, carry):
        hand(off, 0).wait_recv()
        for d in range(groups // 2):
            hand(off, d).wait_send()
        for d in range(1, groups // 2):
            relay(off, d).wait()
        return carry

    lax.fori_loop(0, n, finish, 0)

    def drain(off, carry):
        across(off).wait_send()
        return carry

    lax.fori_loop(1, n, drain, 0)


def spread(blocks, rows, gate_weight, up_weight, groups):
    n, depth, share = blocks.shape
    hidden = jax.ShapeDtypeStruct((rows.shape[0], gate_weight.shape[1]), jnp.float32)
    dma = pltpu.SemaphoreType.DMA
    return pl.pallas_call(
        functools.partial(spread_kernel, n, groups),
        out_shape=(
            jax.ShapeDtypeStruct((n, depth, share * groups), blocks.dtype),
            hidden,
            hidden,
        ),
        in_specs=[VMEM_SPEC, ANY_SPEC, ANY_SPEC, ANY_SPEC],
        out_specs=(VMEM_SPEC, VMEM_SPEC, VMEM_SPEC),
        scratch_shapes=[
            pltpu.VMEM(rows.shape, rows.dtype),
            pltpu.VMEM(gate_weight.shape, gate_weight.dtype),
            pltpu.VMEM(up_weight.shape, up_weight.dtype),
            dma((3,)),
            dma(()),
            dma((n,)),
            dma((n,)),
            dma((groups // 2, n)),
            dma((groups // 2, n)),
            dma((groups // 2 - 1, n)),
            dma((groups // 2 - 1, n)),
        ],
        compiler_params=pltpu.CompilerParams(collective_id=0, has_side_effects=True),
    )(blocks, rows, gate_weight, up_weight)


def collect_kernel(
    n,
    groups,
    part_ref,
    rows_hbm,
    grads_hbm,
    act_hbm,
    gate_hbm,
    up_hbm,
    out_ref,
    gate_out,
    up_out,
    down_out,
    near,
    pair,
    far,
    final,
    rows_ref,
    grads_ref,
    act_ref,
    gate_ref,
    up_ref,
    load_sem,
    s_n,
    r_n,
    s_f,
    r_f,
    s_a,
    r_a,
):
    me = lax.axis_index("sp")
    member, sibling, others = tp_places(groups)
    half = groups // 2
    share = out_ref.shape[2]
    seat, row = lax.rem(member, 2), lax.div(member, 2)
    greet([lax.rem(me + off, n) for off in range(1, n)], [sibling] + others)

    def home(off):
        return lax.rem(me + off, n)

    def to_sibling(off, h):
        return remote(
            part_ref.at[home(off), :, columns(2 * h + 1 - seat, share)],
            near.at[home(off), h],
            s_n.at[h, off],
            r_n.at[h, off],
            tp=sibling,
        )

    def to_other(off, d):
        h = lax.rem(row + d, half)
        return remote(
            pair.at[home(off), h],
            far.at[d - 1, home(off)],
            s_f.at[d - 1, off],
            r_f.at[d - 1, off],
            tp=others[d - 1],
        )

    def to_home(off):
        return remote(
            final.at[home(off)], out_ref.at[me], s_a.at[off], r_a.at[off], sp=home(off)
        )

    def open_step(i, carry):
        off = lax.rem(i + 1, n)
        for h in range(half):
            to_sibling(off, h).start()
        return carry

    lax.fori_loop(0, n, open_step, 0)
    sources = (act_hbm, gate_hbm, up_hbm, rows_hbm, grads_hbm)
    held = (act_ref, gate_ref, up_ref, rows_ref, grads_ref)
    loads = [pltpu.make_async_copy(a, b, load_sem.at[i]) for i, (a, b) in enumerate(zip(sources, held))]
    for load in loads:
        load.start()
    width = rows_ref.shape[1]
    inside = width % (128 * n) == 0
    pieces = n if inside else 8
    size = width // pieces

    def across_rows(a, b):
        total = lax.dot_general(a, b, (((0,), (0,)), ((), ())), preferred_element_type=jnp.float32)
        return total.astype(jnp.bfloat16)

    def weigh(piece):
        at = columns(piece, size)
        rows = rows_ref[:, at]
        gate_out[at, :] = across_rows(rows, gate_ref[...])
        up_out[at, :] = across_rows(rows, up_ref[...])
        down_out[:, at] = across_rows(act_ref[...], grads_ref[:, at])

    def weigh_step(piece, carry):
        weigh(piece)
        return carry

    def pair_step(i, carry):
        off = lax.rem(i + 1, n)
        for h in range(half):
            to_sibling(off, h).wait_recv()
            mine = part_ref[home(off), :, columns(2 * h + seat, share)].astype(jnp.float32)
            total = mine + near[home(off), h].astype(jnp.float32)
            pair[home(off), h] = total.astype(jnp.bfloat16)
        for d in range(1, half):
            to_other(off, d).start()
        return carry

    lax.fori_loop(0, n, pair_step, 0)

    for load in loads:
        load.wait()
    if inside:
        weigh(n - 1)
    else:
        lax.fori_loop(0, pieces, weigh_step, 0)

    def summed(off):
        total = pair[home(off), row].astype(jnp.float32)
        for d in range(1, half):
            to_other(off, d).wait_recv()
            total = total + far[d - 1, home(off)].astype(jnp.float32)
        return total.astype(jnp.bfloat16)

    def home_step(off, carry):
        final[home(off)] = summed(off)
        to_home(off).start()
        if inside:
            weigh(off - 1)
        return carry

    lax.fori_loop(1, n, home_step, 0)
    out_ref[me] = summed(0)

    def drain(off, carry):
        for h in range(half):
            to_sibling(off, h).wait_send()
        for d in range(1, half):
            to_other(off, d).wait_send()
        return carry

    lax.fori_loop(0, n, drain, 0)

    def arrive(off, carry):
        to_home(off).wait()
        return carry

    lax.fori_loop(1, n, arrive, 0)


def collect(parts, rows, grads, act, gate_part, up_part, groups):
    n, depth, width = parts.shape
    ff = act.shape[1]
    share, half = width // groups, groups // 2
    dma = pltpu.SemaphoreType.DMA
    return pl.pallas_call(
        functools.partial(collect_kernel, n, groups),
        out_shape=(
            jax.ShapeDtypeStruct((n, depth, share), parts.dtype),
            jax.ShapeDtypeStruct((width, ff), parts.dtype),
            jax.ShapeDtypeStruct((width, ff), parts.dtype),
            jax.ShapeDtypeStruct((ff, width), parts.dtype),
        ),
        in_specs=[VMEM_SPEC] + [ANY_SPEC] * 5,
        out_specs=(VMEM_SPEC,) * 4,
        scratch_shapes=[
            pltpu.VMEM((n, half, depth, share), parts.dtype),
            pltpu.VMEM((n, half, depth, share), parts.dtype),
            pltpu.VMEM((half - 1, n, depth, share), parts.dtype),
            pltpu.VMEM((n, depth, share), parts.dtype),
            pltpu.VMEM(rows.shape, rows.dtype),
            pltpu.VMEM(grads.shape, grads.dtype),
            pltpu.VMEM(act.shape, act.dtype),
            pltpu.VMEM(act.shape, act.dtype),
            pltpu.VMEM(act.shape, act.dtype),
            dma((5,)),
            dma((half, n)),
            dma((half, n)),
            dma((half - 1, n)),
            dma((half - 1, n)),
            dma((n,)),
            dma((n,)),
        ],
        compiler_params=pltpu.CompilerParams(collective_id=1, has_side_effects=True),
    )(parts, rows, grads, act, gate_part, up_part)


def widen_kernel(groups, chunks, own_ref, out_ref, own_sem, s_f, r_f, s_g, r_g):
    member, sibling, others = tp_places(groups)
    rows, share = own_ref.shape
    size = rows // chunks
    greet([], [sibling] + others)

    def place(c, owner):
        return out_ref.at[pl.ds(c * size, size), columns(owner, share)]

    def hand(c, d):
        target = sibling if d == 0 else others[d - 1]
        return remote(
            own_ref.at[pl.ds(c * size, size)],
            place(c, member),
            s_f.at[d, c],
            r_f.at[d, c],
            tp=target,
        )

    def relay(c, d):
        piece = place(c, others[d - 1])
        return remote(piece, piece, s_g.at[d - 1, c], r_g.at[d - 1, c], tp=sibling)

    for c in range(chunks):
        for d in range(1, groups // 2):
            hand(c, d).start()
    for c in range(chunks):
        hand(c, 0).start()
    own = pltpu.make_async_copy(own_ref, out_ref.at[:, columns(member, share)], own_sem)
    own.start()
    for c in range(chunks):
        for d in range(1, groups // 2):
            hand(c, d).wait_recv()
            relay(c, d).start()
    own.wait()
    for c in range(chunks):
        hand(c, 0).wait_recv()
        for d in range(groups // 2):
            hand(c, d).wait_send()
        for d in range(1, groups // 2):
            relay(c, d).wait()


def widen(own, groups):
    rows, share = own.shape
    chunks = 4 if rows % 64 == 0 else 1
    dma = pltpu.SemaphoreType.DMA
    return pl.pallas_call(
        functools.partial(widen_kernel, groups, chunks),
        out_shape=jax.ShapeDtypeStruct((rows, share * groups), own.dtype),
        in_specs=[VMEM_SPEC],
        out_specs=VMEM_SPEC,
        scratch_shapes=[
            dma(()),
            dma((groups // 2, chunks)),
            dma((groups // 2, chunks)),
            dma((groups // 2 - 1, chunks)),
            dma((groups // 2 - 1, chunks)),
        ],
        compiler_params=pltpu.CompilerParams(collective_id=2, has_side_effects=True),
    )(own)


def fold_kernel(n, part_ref, out_ref, near, pair, far, s_n, r_n, s_f, r_f):
    me = lax.axis_index("sp")
    seat, row = lax.rem(me, 2), lax.div(me, 2)
    partner = me + 1 - 2 * seat
    half = n // 2
    greet([partner] + [lax.rem(me + 2 * d, n) for d in range(1, half)], [])

    def spot(d):
        return lax.rem(row + d, half)

    def to_partner(d):
        return remote(
            part_ref.at[2 * spot(d) + 1 - seat], near.at[d], s_n.at[d], r_n.at[d], sp=partner
        )

    def to_owner(d):
        return remote(
            pair.at[d], far.at[d], s_f.at[d], r_f.at[d], sp=lax.rem(me + 2 * d, n)
        )

    def open_step(i, carry):
        to_partner(lax.rem(i + 1, half)).start()
        return carry

    lax.fori_loop(0, half, open_step, 0)

    def paired(d):
        to_partner(d).wait_recv()
        mine = part_ref[2 * spot(d) + seat].astype(jnp.float32)
        return mine + near[d].astype(jnp.float32)

    def pair_step(d, carry):
        pair[d] = paired(d).astype(jnp.bfloat16)
        to_owner(d).start()
        return carry

    lax.fori_loop(1, half, pair_step, 0)
    out_ref[...] = paired(0)

    def add_step(d, carry):
        to_owner(d).wait_recv()
        out_ref[...] += far[d].astype(jnp.float32)
        return carry

    lax.fori_loop(1, half, add_step, 0)

    def drain(d, carry):
        to_partner(d).wait_send()
        return carry

    lax.fori_loop(0, half, drain, 0)

    def drain_owner(d, carry):
        to_owner(d).wait_send()
        return carry

    lax.fori_loop(1, half, drain_owner, 0)


def fold(parts):
    n, rows, cols = parts.shape
    half = n // 2
    dma = pltpu.SemaphoreType.DMA
    return pl.pallas_call(
        functools.partial(fold_kernel, n),
        out_shape=jax.ShapeDtypeStruct((rows, cols), jnp.float32),
        in_specs=[VMEM_SPEC],
        out_specs=VMEM_SPEC,
        scratch_shapes=[
            pltpu.VMEM((half, rows, cols), parts.dtype),
            pltpu.VMEM((half, rows, cols), parts.dtype),
            pltpu.VMEM((half, rows, cols), parts.dtype),
            dma((half,)),
            dma((half,)),
            dma((half,)),
            dma((half,)),
        ],
        compiler_params=pltpu.CompilerParams(collective_id=3, has_side_effects=True),
    )(parts)


HBM_SPEC = pl.BlockSpec(memory_space=pltpu.HBM)
BF16, F32 = jnp.bfloat16, jnp.float32


def dot_nn(a, b):
    return jnp.dot(a, b, preferred_element_type=F32)


def dot_nt(a, b):
    return lax.dot_general(a, b, (((1,), (1,)), ((), ())), preferred_element_type=F32)


def dot_tn(a, b):
    return lax.dot_general(a, b, (((0,), (0,)), ((), ())), preferred_element_type=F32)


def fused_kernel(
    n,
    groups,
    out_grad_hbm,
    routes_hbm,
    route_weight_hbm,
    conv_input_hbm,
    out_gate_hbm,
    in_gate_hbm,
    taps_hbm,
    rows_hbm,
    wg_hbm,
    wu_hbm,
    dn_hbm,
    ow_hbm,
    gate_out,
    up_out,
    down_out,
    mid_out,
    weight_out,
    input_out,
    out_gate_out,
    in_gate_out,
    out_grad,
    routes,
    route_weight,
    conv_input,
    out_gate,
    in_gate,
    taps,
    rows,
    wgu,
    dn,
    ow,
    hidden,
    place,
    weight,
    picker,
    send,
    grads,
    act,
    parts,
    row_part,
    near,
    pair,
    far,
    final,
    back,
    total,
    wide,
    rim,
    mixed,
    conv,
    gated,
    slices,
    follow,
    later,
    far_routes,
    far_weight,
    far_tokens,
    far_total,
    sum_out,
    sum_in,
    load_sem,
    s_a,
    r_a,
    s_x,
    r_x,
    s_b,
    r_b,
    s_g,
    r_g,
    s_n,
    r_n,
    s_f,
    r_f,
    s_h,
    r_h,
    s_rim,
    r_rim,
    s_d,
    r_d,
    s_p,
    r_p,
    s_c,
    r_c,
    s_e,
    r_e,
    s_t,
    r_t,
    s_m,
    r_m,
    s_mx,
    r_mx,
    s_mr,
    r_mr,
    s_v,
    r_v,
    s_w,
    r_w,
    s_l,
    r_l,
):
    me = lax.axis_index("sp")
    member = lax.axis_index("tp")
    seat = lax.rem(member, 2)
    line = lax.div(member, 2)
    sibling = member + 1 - 2 * seat
    other = lax.rem(member + 2, groups)
    tokens, width = out_grad.shape
    slots = rows.shape[1]
    ff = dn.shape[0]
    share = width // groups
    team = n // 2
    pace = team // 2
    per = n // groups
    span = width // n

    barrier = pltpu.get_barrier_semaphore()

    def call(off, carry):
        pl.semaphore_signal(
            barrier,
            inc=1,
            device_id={"sp": lax.rem(me + off, n)},
            device_id_type=pl.DeviceIdType.MESH,
        )
        return carry

    lax.fori_loop(1, n, call, 0)
    for peer in (sibling, other):
        pl.semaphore_signal(
            barrier, inc=1, device_id={"tp": peer}, device_id_type=pl.DeviceIdType.MESH
        )
    early = [
        pltpu.make_async_copy(routes_hbm, routes, load_sem.at[5]),
        pltpu.make_async_copy(route_weight_hbm, route_weight, load_sem.at[6]),
        pltpu.make_async_copy(out_grad_hbm, out_grad, load_sem.at[7]),
        pltpu.make_async_copy(in_gate_hbm, in_gate, load_sem.at[8]),
        pltpu.make_async_copy(conv_input_hbm, conv_input, load_sem.at[9]),
        pltpu.make_async_copy(out_gate_hbm, out_gate, load_sem.at[10]),
        pltpu.make_async_copy(taps_hbm, taps, load_sem.at[11]),
    ]
    loads = [
        pltpu.make_async_copy(wg_hbm, wgu.at[:, pl.ds(0, ff)], load_sem.at[0]),
        pltpu.make_async_copy(wu_hbm, wgu.at[:, pl.ds(ff, ff)], load_sem.at[1]),
        pltpu.make_async_copy(rows_hbm, rows, load_sem.at[2]),
        pltpu.make_async_copy(dn_hbm, dn, load_sem.at[3]),
        pltpu.make_async_copy(ow_hbm, ow, load_sem.at[4]),
    ]
    for load in early + loads:
        load.start()

    spot = lax.rem(me, team)
    base = me - spot
    mirror = lax.rem(me + team, n)
    partner = me + 1 - 2 * lax.rem(me, 2)

    def taker(k):
        return base + lax.rem(spot + lax.rem(k, team), team)

    def giver(k):
        return base + lax.rem(spot + team - lax.rem(k, team), team)

    def source(k):
        return lax.rem(giver(k) + team * lax.div(k, team), n)

    def owner(k):
        return lax.rem(me + team * lax.div(k, team), n)

    def slice_at(j):
        return pl.ds(pl.multiple_of(j * span, span), span)

    def across(k):
        return remote(
            send.at[k],
            grads.at[owner(k), :, columns(member, share)],
            s_a.at[k],
            r_a.at[k],
            sp=taker(k),
        )

    def hand(k):
        piece = grads.at[source(k), :, columns(member, share)]
        return remote(piece, piece, s_b.at[k], r_b.at[k], tp=sibling)

    def cross(k):
        piece = grads.at[source(k), :, columns(member, share)]
        return remote(piece, piece, s_x.at[k], r_x.at[k], tp=other)

    def relay(k):
        piece = grads.at[source(k), :, columns(other, share)]
        return remote(piece, piece, s_g.at[k], r_g.at[k], tp=sibling)

    def to_sibling(k, h):
        return remote(
            row_part.at[source(k), :, columns(2 * h + 1 - seat, share)],
            near.at[source(k), h],
            s_n.at[h, k],
            r_n.at[h, k],
            tp=sibling,
        )

    def to_other(k):
        return remote(
            pair.at[source(k), 1 - line], far.at[source(k)], s_f.at[k], r_f.at[k], tp=other
        )

    def to_home(k):
        return remote(final.at[source(k)], back.at[k], s_h.at[k], r_h.at[k], sp=giver(k))

    def to_mirror(i):
        sources = (routes, route_weight, out_grad.at[:, columns(member, share)], sum_out)
        landings = (far_routes, far_weight, far_tokens, sum_in)
        return remote(sources[i], landings[i], s_t.at[i], r_t.at[i], sp=mirror)

    def rim_copy(i, ref):
        return remote(
            ref.at[pl.ds(tokens - 16, 16)],
            rim.at[i],
            s_rim.at[i],
            r_rim.at[i],
            sp=lax.rem(me + 1, n),
        )

    def gated_along(q):
        return remote(gated.at[me], gated.at[me], s_d.at[q], r_d.at[q], sp=taker(2 * q))

    def gated_across():
        return remote(gated.at[me], gated.at[me], s_c, r_c, sp=mirror)

    def gated_on(q):
        piece = gated.at[mirror]
        return remote(piece, piece, s_e.at[q], r_e.at[q], sp=taker(2 * q))

    def gated_over(q):
        piece = gated.at[source(2 * q)]
        return remote(piece, piece, s_p.at[q], r_p.at[q], sp=partner)

    for load in early[:2]:
        load.wait()
    first = lax.broadcasted_iota(jnp.int32, (tokens, tokens), 0)
    second = lax.broadcasted_iota(jnp.int32, (tokens, tokens), 1)
    earlier = jnp.where(first < second, 1.0, 0.0).astype(BF16)
    seats = lax.broadcasted_iota(jnp.int32, (slots, tokens), 0).astype(F32)

    def settle_places(named_by, weighed_by):
        names = lax.broadcasted_iota(jnp.int32, (n, tokens), 0)
        chosen = jnp.zeros((n, tokens), jnp.bool_)
        weights = jnp.zeros((n, tokens), F32)
        for choice in range(routes.shape[0]):
            named = names == named_by[choice : choice + 1, :]
            chosen = jnp.logical_or(chosen, named)
            weights = weights + jnp.where(named, weighed_by[choice : choice + 1, :], 0.0)
        marks = jnp.where(chosen, 1.0, 0.0)
        places = jnp.where(chosen, dot_nn(marks.astype(BF16), earlier), -1.0)
        for e in range(n):
            place[e] = places[e : e + 1, :]
            weight[e] = weights[e : e + 1, :]

    def pick(k):
        e = taker(k)
        filled = place[e] == seats
        found = jnp.where(filled, 1.0, 0.0).astype(BF16)
        picker[k] = found
        held = jnp.sum(jnp.where(filled, weight[e], 0.0), axis=1, keepdims=True)
        return found, held

    settle_places(routes, route_weight)
    for load in early[2:]:
        load.wait()
    pl.semaphore_wait(barrier, n + 1)
    for i, ref in enumerate((in_gate, conv_input)):
        rim_copy(i, ref).start()

    for i in range(3):
        to_mirror(i).start()

    def build(k, carry):
        found, held = pick(k)
        own = dot_nn(found, out_grad[:, columns(member, share)])
        send[k] = (held * own).astype(BF16)
        across(k).start()
        return carry

    def build_far(k, carry):
        found, held = pick(k)
        send[k] = (held * dot_nn(found, far_tokens[...])).astype(BF16)
        across(k).start()
        return carry

    lax.fori_loop(1, team, build, 0)
    found, held = pick(0)
    for g in range(groups):
        at = pl.ds(g * share, share)
        grads[me, :, at] = (held * dot_nn(found, out_grad[:, at])).astype(BF16)
    for load in loads[:3]:
        load.wait()
    couples = 2

    def project(c, carry):
        at = pl.ds(c * couples, couples)
        rows_c = rows[at].reshape(couples * slots, width)
        hidden[at] = dot_nn(rows_c, wgu[...]).reshape(couples, slots, 2 * ff)
        return carry

    lax.fori_loop(0, n // couples, project, 0)

    for i, ref in enumerate((in_gate, conv_input)):
        rim_copy(i, ref).wait_recv()
    prior = rim[0].astype(F32) * rim[1].astype(F32)
    mixed[0:16] = jnp.where(me == 0, 0.0, prior)
    mixed[pl.ds(16, tokens)] = in_gate[...].astype(F32) * conv_input[...].astype(F32)
    reach = taps.shape[0]
    conv_sum = taps[0:1, :] * mixed[pl.ds(16, tokens)]
    for tap in range(1, reach):
        conv_sum = conv_sum + taps[tap : tap + 1, :] * mixed[pl.ds(16 - tap, tokens)]
    conv[...] = conv_sum
    gated[me] = (out_gate[...].astype(F32) * conv_sum).astype(BF16)
    for q in range(1, pace):
        gated_along(q).start()
    gated_across().start()
    gated_over(0).start()
    loads[3].wait()
    loads[4].wait()

    def serve():
        for i in range(3):
            to_mirror(i).wait_recv()
        settle_places(far_routes, far_weight)
        lax.fori_loop(team + 1, n, build_far, 0)
        found, held = pick(team)
        grads[mirror, :, columns(member, share)] = (
            held * dot_nn(found, far_tokens[...])
        ).astype(BF16)

    def arrive(k):
        @pl.when(k != team)
        def _():
            across(k).wait_recv()

        cross(k).start()
        hand(k).start()

    def pass_on(k):
        cross(k).wait_recv()
        relay(k).start()

    def backward(k):
        @pl.when(k > 0)
        def _():
            hand(k).wait_recv()
            relay(k).wait_recv()

        s = source(k)
        gate = hidden[s, :, 0:ff]
        up = hidden[s, :, ff : 2 * ff]
        sig = jax.nn.sigmoid(gate)
        act[s] = (gate * sig * up).astype(BF16)
        act_grad = dot_nt(grads[s], dn[...])
        parts[s, :, 0:ff] = (act_grad * up * sig * (1.0 + gate * (1.0 - sig))).astype(BF16)
        parts[s, :, ff : 2 * ff] = (act_grad * gate * sig).astype(BF16)
        both = parts[s]
        for g in range(groups):
            at = pl.ds(g * share, share)
            row_part[s, :, at] = dot_nt(both, wgu[at, :]).astype(BF16)
        for h in range(2):
            to_sibling(k, h).start()

    def pair_up(k):
        s = source(k)
        for h in range(2):
            to_sibling(k, h).wait_recv()
            mine = row_part[s, :, columns(2 * h + seat, share)].astype(F32)
            pair[s, h] = (mine + near[s, h].astype(F32)).astype(BF16)
        to_other(k).start()

    def finish(k):
        s = source(k)
        to_other(k).wait_recv()
        final[s] = (pair[s, line].astype(F32) + far[s].astype(F32)).astype(BF16)

        @pl.when(lax.rem(k, team) > 0)
        def _():
            to_home(k).start()

    def within(p, low, act_on):
        k = jnp.where(p < team - 1, p, jnp.where(p < n - 1, p + 1, team - 1))

        @pl.when(jnp.logical_and(p >= low, p < n))
        def _():
            act_on(k)

    def step(j, carry):
        @pl.when(j == team - 2)
        def _():
            serve()

        @pl.when(j == team - 1)
        def _():
            gated_across().wait_recv()
            for q in range(1, pace):
                gated_on(q).start()
                gated_along(q).wait_recv()
                gated_over(q).start()
            gated_over(pace).start()

        @pl.when(j == n - 1)
        def _():
            for q in range(1, pace):
                gated_on(q).wait_recv()
                gated_over(pace + q).start()

        within(j + 1, 1, arrive)
        within(j, 1, pass_on)
        within(j - 1, 0, backward)
        within(j - 2, 0, pair_up)
        within(j - 3, 0, finish)
        return carry

    lax.fori_loop(0, n + 3, step, 0)

    far_total[...] = dot_tn(picker[team], final[mirror])

    def gather_far(k, carry):
        to_home(k).wait_recv()
        far_total[...] += dot_tn(picker[k], back[k])
        return carry

    lax.fori_loop(team + 1, n, gather_far, 0)
    sum_out[...] = far_total[...].astype(BF16)
    to_mirror(3).start()

    total[...] = out_grad[:, columns(member, share)].astype(F32) + dot_tn(picker[0], final[me])

    def gather_home(k, carry):
        to_home(k).wait_recv()
        total[...] += dot_tn(picker[k], back[k])
        return carry

    lax.fori_loop(1, team, gather_home, 0)
    to_mirror(3).wait_recv()
    mid = (total[...] + sum_in[...].astype(F32)).astype(BF16)
    mid_out[...] = mid
    wide[:, columns(member, share)] = mid

    def mid_sibling():
        piece = wide.at[:, columns(member, share)]
        return remote(piece, piece, s_m, r_m, tp=sibling)

    def mid_other(q):
        piece = wide.at[:, slice_at(member * per + q)]
        return remote(piece, piece, s_mx.at[q], r_mx.at[q], tp=other)

    def mid_relay(q):
        piece = wide.at[:, slice_at(other * per + q)]
        return remote(piece, piece, s_mr.at[q], r_mr.at[q], tp=sibling)

    def slice_out(j):
        return remote(wide.at[:, slice_at(j)], slices.at[me], s_v.at[j], r_v.at[me], sp=j)

    def slice_in(s):
        return remote(wide.at[:, slice_at(me)], slices.at[s], s_v.at[s], r_v.at[s], sp=s)

    def slice_relay(s):
        piece = slices.at[s]
        return remote(piece, piece, s_w.at[s], r_w.at[s], tp=sibling)

    def send_slice(j):
        @pl.when(j != me)
        def _():
            slice_out(j).start()

    for q in range(per):
        mid_other(q).start()
    mid_sibling().start()
    for q in range(per):
        send_slice(member * per + q)

    chunk = 128 if width % 256 else 256
    chunks = width // chunk

    def weigh(piece, carry):
        at = columns(piece, chunk)
        tall = n * slots
        grown = dot_tn(rows[:, :, at].reshape(tall, chunk), parts[...].reshape(tall, 2 * ff))
        gate_out[at, :] = grown[:, 0:ff].astype(BF16)
        up_out[at, :] = grown[:, ff : 2 * ff].astype(BF16)
        down_out[:, at] = dot_tn(
            act[...].reshape(tall, ff), grads[:, :, at].reshape(tall, chunk)
        ).astype(BF16)
        return carry

    lax.fori_loop(0, chunks // 2, weigh, 0)
    for q in range(per):
        mid_other(q).wait_recv()
        mid_relay(q).start()
        send_slice(other * per + q)
    lax.fori_loop(chunks // 2, chunks, weigh, 0)
    mid_sibling().wait_recv()
    for q in range(per):
        mid_relay(q).wait_recv()
    gated_grad = dot_nn(wide[...], ow[...])
    conv_grad = gated_grad * out_gate[...].astype(F32)
    follow[pl.ds(0, tokens)] = conv_grad

    back_rim = remote(
        follow.at[pl.ds(0, 8)], later, s_l, r_l, sp=lax.rem(me + n - 1, n)
    )
    back_rim.start()
    out_gate_out[...] = (gated_grad * conv[...]).astype(BF16)
    for q in range(team):
        gated_over(q).wait_recv()
    weight_out[...] = dot_tn(wide[:, slice_at(me)], gated[me])
    holder = lax.rem(lax.div(me, per), 2)

    def meet(off, carry):
        s = lax.rem(me + off, n)

        @pl.when(holder == seat)
        def _():
            slice_in(s).wait_recv()
            slice_relay(s).start()

        @pl.when(holder != seat)
        def _():
            slice_relay(s).wait_recv()

        weight_out[...] += dot_tn(slices[s], gated[s])
        return carry

    lax.fori_loop(1, n, meet, 0)
    back_rim.wait_recv()
    follow[pl.ds(tokens, 8)] = jnp.where(me == n - 1, 0.0, later[...])
    mixed_grad = taps[0:1, :] * follow[pl.ds(0, tokens)]
    for tap in range(1, reach):
        mixed_grad = mixed_grad + taps[tap : tap + 1, :] * follow[pl.ds(tap, tokens)]
    input_out[...] = (mixed_grad * in_gate[...].astype(F32)).astype(BF16)
    in_gate_out[...] = (mixed_grad * conv_input[...].astype(F32)).astype(BF16)

    def drain(k, carry):
        @pl.when(lax.rem(k, team) > 0)
        def _():
            across(k).wait_send()
            to_home(k).wait_send()

        @pl.when(k > 0)
        def _():
            hand(k).wait_send()
            cross(k).wait_send()
            relay(k).wait_send()

        for h in range(2):
            to_sibling(k, h).wait_send()
        to_other(k).wait_send()
        return carry

    lax.fori_loop(0, n, drain, 0)

    def drain_slices(off, carry):
        s = lax.rem(me + off, n)

        @pl.when(holder == seat)
        def _():
            slice_relay(s).wait_send()

        return carry

    lax.fori_loop(1, n, drain_slices, 0)
    for i, ref in enumerate((in_gate, conv_input)):
        rim_copy(i, ref).wait_send()
    for q in range(team):
        gated_over(q).wait_send()
    for q in range(1, pace):
        gated_along(q).wait_send()
        gated_on(q).wait_send()
    gated_across().wait_send()
    for i in range(4):
        to_mirror(i).wait_send()
    mid_sibling().wait_send()
    back_rim.wait_send()
    for q in range(per):
        mid_other(q).wait_send()
        mid_relay(q).wait_send()
        for owner in (member, other):

            @pl.when(owner * per + q != me)
            def _():
                slice_out(owner * per + q).wait_send()


def settle_kernel(count, *refs):
    sources, targets, sem = refs[:count], refs[count : 2 * count], refs[2 * count]
    moves = [pltpu.make_async_copy(a, b, sem.at[i]) for i, (a, b) in enumerate(zip(sources, targets))]
    for move in moves:
        move.start()
    for move in moves:
        move.wait()


def settle(arrays):
    count = len(arrays)
    return pl.pallas_call(
        functools.partial(settle_kernel, count),
        out_shape=tuple(jax.ShapeDtypeStruct(a.shape, a.dtype) for a in arrays),
        in_specs=[ANY_SPEC] * count,
        out_specs=(HBM_SPEC,) * count,
        scratch_shapes=[pltpu.SemaphoreType.DMA((count,))],
        compiler_params=pltpu.CompilerParams(vmem_limit_bytes=2**20),
    )(*arrays)


def fused(
    out_grad,
    routes,
    route_weight,
    rows,
    gate_weight,
    up_weight,
    down_weight,
    conv_input,
    out_gate,
    in_gate,
    taps,
    out_weight,
    groups,
):
    n, slots, width = rows.shape
    tokens = out_grad.shape[0]
    ff = gate_weight.shape[1]
    chans = conv_input.shape[1]
    share, span, team, per = width // groups, width // n, n // 2, n // groups
    dma = pltpu.SemaphoreType.DMA

    def held(*shape):
        return pltpu.VMEM(shape, BF16)

    def exact(*shape):
        return pltpu.VMEM(shape, F32)

    operands = (
        out_grad,
        routes.T,
        route_weight.T,
        conv_input,
        out_gate,
        in_gate,
        taps,
        rows,
        gate_weight,
        up_weight,
        down_weight,
        out_weight,
    )
    small = held(tokens, chans)
    return pl.pallas_call(
        functools.partial(fused_kernel, n, groups),
        out_shape=(
            held(width, ff),
            held(width, ff),
            held(ff, width),
            held(tokens, share),
            exact(span, chans),
            small,
            small,
            small,
        ),
        in_specs=[HBM_SPEC] * 12,
        out_specs=(VMEM_SPEC,) * 8,
        scratch_shapes=[
            held(tokens, width),
            pltpu.VMEM(routes.T.shape, routes.dtype),
            exact(*route_weight.T.shape),
            held(tokens, chans),
            held(tokens, chans),
            held(tokens, chans),
            exact(*taps.shape),
            held(n, slots, width),
            held(width, 2 * ff),
            held(ff, width),
            held(width, chans),
            exact(n, slots, 2 * ff),
            exact(n, 1, tokens),
            exact(n, 1, tokens),
            held(n, slots, tokens),
            held(n, slots, share),
            held(n, slots, width),
            held(n, slots, ff),
            held(n, slots, 2 * ff),
            held(n, slots, width),
            held(n, 2, slots, share),
            held(n, 2, slots, share),
            held(n, slots, share),
            held(n, slots, share),
            held(n, slots, share),
            exact(tokens, share),
            held(tokens, width),
            held(2, 16, chans),
            exact(16 + tokens, chans),
            exact(tokens, chans),
            held(n, tokens, chans),
            held(n, tokens, span),
            exact(tokens + 8, chans),
            exact(8, chans),
            pltpu.VMEM(routes.T.shape, routes.dtype),
            exact(*route_weight.T.shape),
            held(tokens, share),
            exact(tokens, share),
            held(tokens, share),
            held(tokens, share),
            dma((12,)),
        ]
        + [dma((n,))] * 8
        + [dma((2, n))] * 2
        + [dma((n,))] * 4
        + [dma((2,))] * 2
        + [dma((team,))] * 4
        + [dma(())] * 2
        + [dma((team,))] * 2
        + [dma((4,))] * 2
        + [dma(())] * 2
        + [dma((per,))] * 4
        + [dma((n,))] * 4
        + [dma(())] * 2,
        compiler_params=pltpu.CompilerParams(
            collective_id=4, has_side_effects=True, vmem_limit_bytes=40 * 2**20
        ),
    )(*(pltpu.with_memory_space_constraint(a, pltpu.HBM) for a in operands))


def fits_fused(tokens, slots, width, sources, groups):
    tidy = slots % 16 == 0 and tokens % 16 == 0 and width % (128 * sources) == 0
    return tidy and groups == 4 and sources % 4 == 0


def on_device(
    out_grad,
    routes,
    route_weight,
    expert_rows,
    gate_weight,
    up_weight,
    down_weight,
    conv_input,
    out_gate,
    in_gate,
    taps,
    out_weight,
):
    groups = lax.axis_size("tp")
    sources = lax.axis_size("sp")
    slots, width = expert_rows.shape[2:]
    assert gate_weight.shape[0] == 1
    if not fits_fused(out_grad.shape[0], slots, width, sources, groups):
        return staged(
            out_grad,
            routes,
            route_weight,
            expert_rows,
            gate_weight,
            up_weight,
            down_weight,
            conv_input,
            out_gate,
            in_gate,
            taps,
            out_weight,
        )
    outs = fused(
        out_grad,
        routes,
        route_weight,
        expert_rows.reshape(sources, slots, width),
        gate_weight[0],
        up_weight[0],
        down_weight[0],
        conv_input,
        out_gate,
        in_gate,
        taps,
        out_weight,
        groups,
    )
    outs = settle(outs)
    return tuple(out[None] for out in outs[:3]) + tuple(outs[3:])


def staged(
    out_grad,
    routes,
    route_weight,
    expert_rows,
    gate_weight,
    up_weight,
    down_weight,
    conv_input,
    out_gate,
    in_gate,
    taps,
    out_weight,
):
    groups = lax.axis_size("tp")
    member = lax.axis_index("tp")
    sources = lax.axis_size("sp")
    tok_rows, width = out_grad.shape
    top = routes.shape[1]
    local = gate_weight.shape[0]
    assert local == 1
    experts = local * sources
    slots = expert_rows.shape[2]
    share = width // groups
    own_cols = lax.dynamic_slice_in_dim(out_grad, member * share, share, 1)
    names = jnp.arange(experts, dtype=jnp.int32)
    named = routes[:, :, None] == names[None, None, :]
    chosen = jnp.any(named, axis=1)
    weight = jnp.sum(jnp.where(named, route_weight[:, :, None], 0.0), axis=1)
    order = jnp.arange(tok_rows, dtype=jnp.int32)
    earlier = (order[:, None] > order[None, :]).astype(jnp.bfloat16)
    place = jnp.dot(
        earlier, chosen.astype(jnp.bfloat16), preferred_element_type=jnp.float32
    ).astype(jnp.int32)
    place = jnp.where(chosen, place, -1).T
    filled = place[:, None, :] == jnp.arange(slots, dtype=jnp.int32)[None, :, None]
    slot_weight = jnp.sum(jnp.where(filled, weight.T[:, None, :], 0.0), axis=2)
    picker = filled.astype(jnp.bfloat16).reshape(experts * slots, tok_rows)
    outgoing = jnp.dot(picker, own_cols, preferred_element_type=jnp.float32)
    outgoing = (slot_weight.reshape(-1, 1) * outgoing).astype(jnp.bfloat16)
    outgoing = outgoing.reshape(sources, local * slots, share)
    rows = expert_rows.reshape(-1, width)
    wide_gate, wide_up, tall_down = gate_weight[0], up_weight[0], down_weight[0]
    grads, gate, up = spread(outgoing, rows, wide_gate, wide_up, groups)
    grads = grads.reshape(-1, width)
    sig = jax.nn.sigmoid(gate)
    act = (gate * sig * up).astype(jnp.bfloat16)
    act_grad = lax.dot_general(
        grads, tall_down, (((1,), (1,)), ((), ())), preferred_element_type=jnp.float32
    )
    up_part = (act_grad * gate * sig).astype(jnp.bfloat16)
    gate_part = (act_grad * up * sig * (1.0 + gate * (1.0 - sig))).astype(jnp.bfloat16)
    row_part = lax.dot_general(
        gate_part, wide_gate, (((1,), (1,)), ((), ())), preferred_element_type=jnp.float32
    )
    row_part = row_part + lax.dot_general(
        up_part, wide_up, (((1,), (1,)), ((), ())), preferred_element_type=jnp.float32
    )
    row_part = row_part.astype(jnp.bfloat16).reshape(sources, slots, width)
    returned, gate_grad, up_grad, down_grad = collect(
        row_part, rows, grads, act, gate_part, up_part, groups
    )
    returned = returned.reshape(experts * slots, share)
    gate_grad, up_grad, down_grad = gate_grad[None], up_grad[None], down_grad[None]
    picked = lax.dot_general(
        picker, returned, (((0,), (0,)), ((), ())), preferred_element_type=jnp.float32
    )
    mid_grad = (own_cols.astype(jnp.float32) + picked).astype(jnp.bfloat16)
    mid_whole = widen(mid_grad, groups)
    reach = taps.shape[0] - 1
    rims = jnp.stack([in_gate[tok_rows - reach :], conv_input[tok_rows - reach :]])
    prior = passed_along(rims, "sp", 1)
    mixed = in_gate.astype(jnp.float32) * conv_input.astype(jnp.float32)
    prior_mixed = prior[0].astype(jnp.float32) * prior[1].astype(jnp.float32)
    extended = jnp.concatenate([prior_mixed, mixed], axis=0)
    conv = jnp.zeros_like(mixed)
    for tap in range(reach + 1):
        conv = conv + taps[tap][None, :] * extended[reach - tap : reach - tap + tok_rows]
    gated = (out_gate.astype(jnp.float32) * conv).astype(jnp.bfloat16)
    partial_grad = lax.dot_general(
        mid_whole, gated, (((0,), (0,)), ((), ())), preferred_element_type=jnp.float32
    ).astype(jnp.bfloat16)
    out_weight_grad = fold(partial_grad.reshape(sources, width // sources, gated.shape[1]))
    gated_grad = jnp.dot(mid_whole, out_weight, preferred_element_type=jnp.float32)
    out_gate_grad = (gated_grad * conv).astype(jnp.bfloat16)
    conv_grad = gated_grad * out_gate.astype(jnp.float32)
    later = passed_along(conv_grad[:reach], "sp", -1)
    following = jnp.concatenate([conv_grad, later], axis=0)
    mixed_grad = jnp.zeros_like(conv_grad)
    for tap in range(reach + 1):
        mixed_grad = mixed_grad + taps[tap][None, :] * following[tap : tap + tok_rows]
    input_grad = (mixed_grad * in_gate.astype(jnp.float32)).astype(jnp.bfloat16)
    in_gate_grad = (mixed_grad * conv_input.astype(jnp.float32)).astype(jnp.bfloat16)
    return (
        gate_grad,
        up_grad,
        down_grad,
        mid_grad,
        out_weight_grad,
        input_grad,
        out_gate_grad,
        in_gate_grad,
    )


def solution(mesh):
    in_specs = (
        P("sp", None),
        P("sp", None),
        P("sp", None),
        P(None, "sp", None, None),
        P("sp", None, "tp"),
        P("sp", None, "tp"),
        P("sp", "tp", None),
        P("sp", "tp"),
        P("sp", "tp"),
        P("sp", "tp"),
        P(None, "tp"),
        P(None, "tp"),
    )
    out_specs = (
        P("sp", None, "tp"),
        P("sp", None, "tp"),
        P("sp", "tp", None),
        P("sp", "tp"),
        P("sp", "tp"),
        P("sp", "tp"),
        P("sp", "tp"),
        P("sp", "tp"),
    )
    return jax.shard_map(
        on_device, mesh=mesh, in_specs=in_specs, out_specs=out_specs, check_vma=False
    )
```

```python
import functools

import jax
import jax.numpy as jnp
from jax import lax
from jax.experimental import pallas as pl
from jax.experimental.pallas import tpu as pltpu
from jax.sharding import PartitionSpec as P

ANY_SPEC = pl.BlockSpec(memory_space=pl.ANY)
VMEM_SPEC = pl.BlockSpec(memory_space=pltpu.VMEM)


def passed_along(shard, axis, by):
    peers = lax.axis_size(axis)
    pairs = [(i, i + by) for i in range(peers) if 0 <= i + by < peers]
    return lax.ppermute(shard, axis, pairs)


def remote(src, dst, send_sem, recv_sem, **target):
    return pltpu.make_async_remote_copy(
        src_ref=src,
        dst_ref=dst,
        send_sem=send_sem,
        recv_sem=recv_sem,
        device_id=target,
        device_id_type=pl.DeviceIdType.MESH,
    )


def greet(sp_peers, tp_peers):
    barrier = pltpu.get_barrier_semaphore()
    for peer in sp_peers:
        pl.semaphore_signal(
            barrier, inc=1, device_id={"sp": peer}, device_id_type=pl.DeviceIdType.MESH
        )
    for peer in tp_peers:
        pl.semaphore_signal(
            barrier, inc=1, device_id={"tp": peer}, device_id_type=pl.DeviceIdType.MESH
        )
    pl.semaphore_wait(barrier, len(sp_peers) + len(tp_peers))


def tp_places(groups):
    member = lax.axis_index("tp")
    sibling = member + 1 - 2 * lax.rem(member, 2)
    others = [lax.rem(member + 2 * d, groups) for d in range(1, groups // 2)]
    return member, sibling, others


def columns(member, share):
    return pl.ds(pl.multiple_of(member * share, share), share)


def spread_kernel(
    n,
    groups,
    send_ref,
    rows_hbm,
    wg_hbm,
    wu_hbm,
    out_ref,
    gate_ref,
    up_ref,
    rows_ref,
    wg_ref,
    wu_ref,
    load_sem,
    own_sem,
    s_a,
    r_a,
    s_f,
    r_f,
    s_g,
    r_g,
):
    me = lax.axis_index("sp")
    member, sibling, others = tp_places(groups)
    share = send_ref.shape[2]
    greet([lax.rem(me + off, n) for off in range(1, n)], [sibling] + others)

    def across(off):
        dest = lax.rem(me + off, n)
        return remote(
            send_ref.at[dest],
            out_ref.at[me, :, columns(member, share)],
            s_a.at[off],
            r_a.at[off],
            sp=dest,
        )

    def block(off, owner):
        return out_ref.at[lax.rem(me + n - off, n), :, columns(owner, share)]

    def hand(off, d):
        target = sibling if d == 0 else others[d - 1]
        return remote(
            block(off, member), block(off, member), s_f.at[d, off], r_f.at[d, off], tp=target
        )

    def relay(off, d):
        piece = block(off, others[d - 1])
        return remote(piece, piece, s_g.at[d - 1, off], r_g.at[d - 1, off], tp=sibling)

    def hand_on(off):
        for d in range(groups // 2):
            hand(off, d).start()

    def relay_on(off):
        for d in range(1, groups // 2):
            hand(off, d).wait_recv()
            relay(off, d).start()

    own = pltpu.make_async_copy(send_ref.at[me], out_ref.at[me, :, columns(member, share)], own_sem)
    own.start()

    def send_out(off, carry):
        across(off).start()
        return carry

    lax.fori_loop(1, n, send_out, 0)
    loads = [
        pltpu.make_async_copy(wg_hbm, wg_ref, load_sem.at[0]),
        pltpu.make_async_copy(wu_hbm, wu_ref, load_sem.at[1]),
        pltpu.make_async_copy(rows_hbm, rows_ref, load_sem.at[2]),
    ]
    for load in loads:
        load.start()
    own.wait()
    hand_on(0)
    tall = rows_ref.shape[0]
    inside = (tall // n) % 16 == 0
    pieces = n if inside else 4
    size = tall // pieces

    def project(piece):
        at = pl.ds(pl.multiple_of(piece * size, size), size)
        rows = rows_ref[at, :]
        gate_ref[at, :] = jnp.dot(rows, wg_ref[...], preferred_element_type=jnp.float32)
        up_ref[at, :] = jnp.dot(rows, wu_ref[...], preferred_element_type=jnp.float32)

    def project_step(piece, carry):
        project(piece)
        return carry

    for load in loads:
        load.wait()
    if inside:
        project(n - 1)
    else:
        lax.fori_loop(0, pieces, project_step, 0)

    def step(off, carry):
        across(off).wait_recv()
        hand_on(off)
        relay_on(off - 1)
        if inside:
            project(off - 1)
        return carry

    lax.fori_loop(1, n, step, 0)
    relay_on(n - 1)

    def finish(off, carry):
        hand(off, 0).wait_recv()
        for d in range(groups // 2):
            hand(off, d).wait_send()
        for d in range(1, groups // 2):
            relay(off, d).wait()
        return carry

    lax.fori_loop(0, n, finish, 0)

    def drain(off, carry):
        across(off).wait_send()
        return carry

    lax.fori_loop(1, n, drain, 0)


def spread(blocks, rows, gate_weight, up_weight, groups):
    n, depth, share = blocks.shape
    hidden = jax.ShapeDtypeStruct((rows.shape[0], gate_weight.shape[1]), jnp.float32)
    dma = pltpu.SemaphoreType.DMA
    return pl.pallas_call(
        functools.partial(spread_kernel, n, groups),
        out_shape=(
            jax.ShapeDtypeStruct((n, depth, share * groups), blocks.dtype),
            hidden,
            hidden,
        ),
        in_specs=[VMEM_SPEC, ANY_SPEC, ANY_SPEC, ANY_SPEC],
        out_specs=(VMEM_SPEC, VMEM_SPEC, VMEM_SPEC),
        scratch_shapes=[
            pltpu.VMEM(rows.shape, rows.dtype),
            pltpu.VMEM(gate_weight.shape, gate_weight.dtype),
            pltpu.VMEM(up_weight.shape, up_weight.dtype),
            dma((3,)),
            dma(()),
            dma((n,)),
            dma((n,)),
            dma((groups // 2, n)),
            dma((groups // 2, n)),
            dma((groups // 2 - 1, n)),
            dma((groups // 2 - 1, n)),
        ],
        compiler_params=pltpu.CompilerParams(collective_id=0, has_side_effects=True),
    )(blocks, rows, gate_weight, up_weight)


def collect_kernel(
    n,
    groups,
    part_ref,
    rows_hbm,
    grads_hbm,
    act_hbm,
    gate_hbm,
    up_hbm,
    out_ref,
    gate_out,
    up_out,
    down_out,
    near,
    pair,
    far,
    final,
    rows_ref,
    grads_ref,
    act_ref,
    gate_ref,
    up_ref,
    load_sem,
    s_n,
    r_n,
    s_f,
    r_f,
    s_a,
    r_a,
):
    me = lax.axis_index("sp")
    member, sibling, others = tp_places(groups)
    half = groups // 2
    share = out_ref.shape[2]
    seat, row = lax.rem(member, 2), lax.div(member, 2)
    greet([lax.rem(me + off, n) for off in range(1, n)], [sibling] + others)

    def home(off):
        return lax.rem(me + off, n)

    def to_sibling(off, h):
        return remote(
            part_ref.at[home(off), :, columns(2 * h + 1 - seat, share)],
            near.at[home(off), h],
            s_n.at[h, off],
            r_n.at[h, off],
            tp=sibling,
        )

    def to_other(off, d):
        h = lax.rem(row + d, half)
        return remote(
            pair.at[home(off), h],
            far.at[d - 1, home(off)],
            s_f.at[d - 1, off],
            r_f.at[d - 1, off],
            tp=others[d - 1],
        )

    def to_home(off):
        return remote(
            final.at[home(off)], out_ref.at[me], s_a.at[off], r_a.at[off], sp=home(off)
        )

    def open_step(i, carry):
        off = lax.rem(i + 1, n)
        for h in range(half):
            to_sibling(off, h).start()
        return carry

    lax.fori_loop(0, n, open_step, 0)
    sources = (act_hbm, gate_hbm, up_hbm, rows_hbm, grads_hbm)
    held = (act_ref, gate_ref, up_ref, rows_ref, grads_ref)
    loads = [pltpu.make_async_copy(a, b, load_sem.at[i]) for i, (a, b) in enumerate(zip(sources, held))]
    for load in loads:
        load.start()
    width = rows_ref.shape[1]
    inside = width % (128 * n) == 0
    pieces = n if inside else 8
    size = width // pieces

    def across_rows(a, b):
        total = lax.dot_general(a, b, (((0,), (0,)), ((), ())), preferred_element_type=jnp.float32)
        return total.astype(jnp.bfloat16)

    def weigh(piece):
        at = columns(piece, size)
        rows = rows_ref[:, at]
        gate_out[at, :] = across_rows(rows, gate_ref[...])
        up_out[at, :] = across_rows(rows, up_ref[...])
        down_out[:, at] = across_rows(act_ref[...], grads_ref[:, at])

    def weigh_step(piece, carry):
        weigh(piece)
        return carry

    def pair_step(i, carry):
        off = lax.rem(i + 1, n)
        for h in range(half):
            to_sibling(off, h).wait_recv()
            mine = part_ref[home(off), :, columns(2 * h + seat, share)].astype(jnp.float32)
            total = mine + near[home(off), h].astype(jnp.float32)
            pair[home(off), h] = total.astype(jnp.bfloat16)
        for d in range(1, half):
            to_other(off, d).start()
        return carry

    lax.fori_loop(0, n, pair_step, 0)

    for load in loads:
        load.wait()
    if inside:
        weigh(n - 1)
    else:
        lax.fori_loop(0, pieces, weigh_step, 0)

    def summed(off):
        total = pair[home(off), row].astype(jnp.float32)
        for d in range(1, half):
            to_other(off, d).wait_recv()
            total = total + far[d - 1, home(off)].astype(jnp.float32)
        return total.astype(jnp.bfloat16)

    def home_step(off, carry):
        final[home(off)] = summed(off)
        to_home(off).start()
        if inside:
            weigh(off - 1)
        return carry

    lax.fori_loop(1, n, home_step, 0)
    out_ref[me] = summed(0)

    def drain(off, carry):
        for h in range(half):
            to_sibling(off, h).wait_send()
        for d in range(1, half):
            to_other(off, d).wait_send()
        return carry

    lax.fori_loop(0, n, drain, 0)

    def arrive(off, carry):
        to_home(off).wait()
        return carry

    lax.fori_loop(1, n, arrive, 0)


def collect(parts, rows, grads, act, gate_part, up_part, groups):
    n, depth, width = parts.shape
    ff = act.shape[1]
    share, half = width // groups, groups // 2
    dma = pltpu.SemaphoreType.DMA
    return pl.pallas_call(
        functools.partial(collect_kernel, n, groups),
        out_shape=(
            jax.ShapeDtypeStruct((n, depth, share), parts.dtype),
            jax.ShapeDtypeStruct((width, ff), parts.dtype),
            jax.ShapeDtypeStruct((width, ff), parts.dtype),
            jax.ShapeDtypeStruct((ff, width), parts.dtype),
        ),
        in_specs=[VMEM_SPEC] + [ANY_SPEC] * 5,
        out_specs=(VMEM_SPEC,) * 4,
        scratch_shapes=[
            pltpu.VMEM((n, half, depth, share), parts.dtype),
            pltpu.VMEM((n, half, depth, share), parts.dtype),
            pltpu.VMEM((half - 1, n, depth, share), parts.dtype),
            pltpu.VMEM((n, depth, share), parts.dtype),
            pltpu.VMEM(rows.shape, rows.dtype),
            pltpu.VMEM(grads.shape, grads.dtype),
            pltpu.VMEM(act.shape, act.dtype),
            pltpu.VMEM(act.shape, act.dtype),
            pltpu.VMEM(act.shape, act.dtype),
            dma((5,)),
            dma((half, n)),
            dma((half, n)),
            dma((half - 1, n)),
            dma((half - 1, n)),
            dma((n,)),
            dma((n,)),
        ],
        compiler_params=pltpu.CompilerParams(collective_id=1, has_side_effects=True),
    )(parts, rows, grads, act, gate_part, up_part)


def widen_kernel(groups, chunks, own_ref, out_ref, own_sem, s_f, r_f, s_g, r_g):
    member, sibling, others = tp_places(groups)
    rows, share = own_ref.shape
    size = rows // chunks
    greet([], [sibling] + others)

    def place(c, owner):
        return out_ref.at[pl.ds(c * size, size), columns(owner, share)]

    def hand(c, d):
        target = sibling if d == 0 else others[d - 1]
        return remote(
            own_ref.at[pl.ds(c * size, size)],
            place(c, member),
            s_f.at[d, c],
            r_f.at[d, c],
            tp=target,
        )

    def relay(c, d):
        piece = place(c, others[d - 1])
        return remote(piece, piece, s_g.at[d - 1, c], r_g.at[d - 1, c], tp=sibling)

    for c in range(chunks):
        for d in range(1, groups // 2):
            hand(c, d).start()
    for c in range(chunks):
        hand(c, 0).start()
    own = pltpu.make_async_copy(own_ref, out_ref.at[:, columns(member, share)], own_sem)
    own.start()
    for c in range(chunks):
        for d in range(1, groups // 2):
            hand(c, d).wait_recv()
            relay(c, d).start()
    own.wait()
    for c in range(chunks):
        hand(c, 0).wait_recv()
        for d in range(groups // 2):
            hand(c, d).wait_send()
        for d in range(1, groups // 2):
            relay(c, d).wait()


def widen(own, groups):
    rows, share = own.shape
    chunks = 4 if rows % 64 == 0 else 1
    dma = pltpu.SemaphoreType.DMA
    return pl.pallas_call(
        functools.partial(widen_kernel, groups, chunks),
        out_shape=jax.ShapeDtypeStruct((rows, share * groups), own.dtype),
        in_specs=[VMEM_SPEC],
        out_specs=VMEM_SPEC,
        scratch_shapes=[
            dma(()),
            dma((groups // 2, chunks)),
            dma((groups // 2, chunks)),
            dma((groups // 2 - 1, chunks)),
            dma((groups // 2 - 1, chunks)),
        ],
        compiler_params=pltpu.CompilerParams(collective_id=2, has_side_effects=True),
    )(own)


def fold_kernel(n, part_ref, out_ref, near, pair, far, s_n, r_n, s_f, r_f):
    me = lax.axis_index("sp")
    seat, row = lax.rem(me, 2), lax.div(me, 2)
    partner = me + 1 - 2 * seat
    half = n // 2
    greet([partner] + [lax.rem(me + 2 * d, n) for d in range(1, half)], [])

    def spot(d):
        return lax.rem(row + d, half)

    def to_partner(d):
        return remote(
            part_ref.at[2 * spot(d) + 1 - seat], near.at[d], s_n.at[d], r_n.at[d], sp=partner
        )

    def to_owner(d):
        return remote(
            pair.at[d], far.at[d], s_f.at[d], r_f.at[d], sp=lax.rem(me + 2 * d, n)
        )

    def open_step(i, carry):
        to_partner(lax.rem(i + 1, half)).start()
        return carry

    lax.fori_loop(0, half, open_step, 0)

    def paired(d):
        to_partner(d).wait_recv()
        mine = part_ref[2 * spot(d) + seat].astype(jnp.float32)
        return mine + near[d].astype(jnp.float32)

    def pair_step(d, carry):
        pair[d] = paired(d).astype(jnp.bfloat16)
        to_owner(d).start()
        return carry

    lax.fori_loop(1, half, pair_step, 0)
    out_ref[...] = paired(0)

    def add_step(d, carry):
        to_owner(d).wait_recv()
        out_ref[...] += far[d].astype(jnp.float32)
        return carry

    lax.fori_loop(1, half, add_step, 0)

    def drain(d, carry):
        to_partner(d).wait_send()
        return carry

    lax.fori_loop(0, half, drain, 0)

    def drain_owner(d, carry):
        to_owner(d).wait_send()
        return carry

    lax.fori_loop(1, half, drain_owner, 0)


def fold(parts):
    n, rows, cols = parts.shape
    half = n // 2
    dma = pltpu.SemaphoreType.DMA
    return pl.pallas_call(
        functools.partial(fold_kernel, n),
        out_shape=jax.ShapeDtypeStruct((rows, cols), jnp.float32),
        in_specs=[VMEM_SPEC],
        out_specs=VMEM_SPEC,
        scratch_shapes=[
            pltpu.VMEM((half, rows, cols), parts.dtype),
            pltpu.VMEM((half, rows, cols), parts.dtype),
            pltpu.VMEM((half, rows, cols), parts.dtype),
            dma((half,)),
            dma((half,)),
            dma((half,)),
            dma((half,)),
        ],
        compiler_params=pltpu.CompilerParams(collective_id=3, has_side_effects=True),
    )(parts)


HBM_SPEC = pl.BlockSpec(memory_space=pltpu.HBM)
BF16, F32 = jnp.bfloat16, jnp.float32


def dot_nn(a, b):
    return jnp.dot(a, b, preferred_element_type=F32)


def dot_nt(a, b):
    return lax.dot_general(a, b, (((1,), (1,)), ((), ())), preferred_element_type=F32)


def dot_tn(a, b):
    return lax.dot_general(a, b, (((0,), (0,)), ((), ())), preferred_element_type=F32)


def fused_kernel(
    n,
    groups,
    out_grad_hbm,
    routes_hbm,
    route_weight_hbm,
    conv_input_hbm,
    out_gate_hbm,
    in_gate_hbm,
    taps_hbm,
    rows_hbm,
    wg_hbm,
    wu_hbm,
    dn_hbm,
    ow_hbm,
    gate_out,
    up_out,
    down_out,
    mid_out,
    weight_out,
    input_out,
    out_gate_out,
    in_gate_out,
    out_grad,
    routes,
    route_weight,
    conv_input,
    out_gate,
    in_gate,
    taps,
    rows,
    wgu,
    dn,
    ow,
    hidden,
    place,
    weight,
    picker,
    send,
    grads,
    act,
    parts,
    row_part,
    near,
    pair,
    far,
    final,
    back,
    total,
    wide,
    rim,
    mixed,
    conv,
    gated,
    slices,
    follow,
    later,
    load_sem,
    s_a,
    r_a,
    s_x,
    r_x,
    s_b,
    r_b,
    s_g,
    r_g,
    s_n,
    r_n,
    s_f,
    r_f,
    s_h,
    r_h,
    s_rim,
    r_rim,
    s_d,
    r_d,
    s_p,
    r_p,
    s_m,
    r_m,
    s_mx,
    r_mx,
    s_mr,
    r_mr,
    s_v,
    r_v,
    s_w,
    r_w,
    s_l,
    r_l,
):
    me = lax.axis_index("sp")
    member = lax.axis_index("tp")
    seat = lax.rem(member, 2)
    line = lax.div(member, 2)
    sibling = member + 1 - 2 * seat
    other = lax.rem(member + 2, groups)
    tokens, width = out_grad.shape
    slots = rows.shape[1]
    ff = dn.shape[0]
    share = width // groups
    deep = n // 2
    per = n // groups
    span = width // n

    barrier = pltpu.get_barrier_semaphore()

    def call(off, carry):
        pl.semaphore_signal(
            barrier,
            inc=1,
            device_id={"sp": lax.rem(me + off, n)},
            device_id_type=pl.DeviceIdType.MESH,
        )
        return carry

    lax.fori_loop(1, n, call, 0)
    for peer in (sibling, other):
        pl.semaphore_signal(
            barrier, inc=1, device_id={"tp": peer}, device_id_type=pl.DeviceIdType.MESH
        )
    early = [
        pltpu.make_async_copy(routes_hbm, routes, load_sem.at[5]),
        pltpu.make_async_copy(route_weight_hbm, route_weight, load_sem.at[6]),
        pltpu.make_async_copy(out_grad_hbm, out_grad, load_sem.at[7]),
        pltpu.make_async_copy(in_gate_hbm, in_gate, load_sem.at[8]),
        pltpu.make_async_copy(conv_input_hbm, conv_input, load_sem.at[9]),
        pltpu.make_async_copy(out_gate_hbm, out_gate, load_sem.at[10]),
        pltpu.make_async_copy(taps_hbm, taps, load_sem.at[11]),
    ]
    loads = [
        pltpu.make_async_copy(wg_hbm, wgu.at[:, pl.ds(0, ff)], load_sem.at[0]),
        pltpu.make_async_copy(wu_hbm, wgu.at[:, pl.ds(ff, ff)], load_sem.at[1]),
        pltpu.make_async_copy(rows_hbm, rows, load_sem.at[2]),
        pltpu.make_async_copy(dn_hbm, dn, load_sem.at[3]),
        pltpu.make_async_copy(ow_hbm, ow, load_sem.at[4]),
    ]
    for load in early + loads:
        load.start()

    def shift(k, way):
        q = lax.div(k, 2)
        step = lax.div(q + 1, 2) * (2 * lax.rem(q, 2) - 1) * way
        deeper = lax.rem(lax.div(me, 2) + step + deep, deep)
        side = lax.rem(lax.rem(me, 2) + lax.rem(k, 2), 2)
        return 2 * deeper + side

    def dest(k):
        return shift(k, 1)

    def source(k):
        return shift(k, -1)

    def slice_at(j):
        return pl.ds(pl.multiple_of(j * span, span), span)

    def across(k):
        return remote(
            send.at[dest(k)],
            grads.at[me, :, columns(member, share)],
            s_a.at[k],
            r_a.at[k],
            sp=dest(k),
        )

    def hand(k):
        piece = grads.at[source(k), :, columns(member, share)]
        return remote(piece, piece, s_b.at[k], r_b.at[k], tp=sibling)

    def cross(k):
        piece = grads.at[source(k), :, columns(member, share)]
        return remote(piece, piece, s_x.at[k], r_x.at[k], tp=other)

    def relay(k):
        piece = grads.at[source(k), :, columns(other, share)]
        return remote(piece, piece, s_g.at[k], r_g.at[k], tp=sibling)

    def to_sibling(k, h):
        return remote(
            row_part.at[source(k), :, columns(2 * h + 1 - seat, share)],
            near.at[source(k), h],
            s_n.at[h, k],
            r_n.at[h, k],
            tp=sibling,
        )

    def to_other(k):
        return remote(
            pair.at[source(k), 1 - line], far.at[source(k)], s_f.at[k], r_f.at[k], tp=other
        )

    def to_home(k):
        return remote(final.at[source(k)], back.at[me], s_h.at[k], r_h.at[k], sp=source(k))

    def rim_copy(i, ref):
        return remote(
            ref.at[pl.ds(tokens - 16, 16)],
            rim.at[i],
            s_rim.at[i],
            r_rim.at[i],
            sp=lax.rem(me + 1, n),
        )

    def gated_along(q):
        return remote(gated.at[me], gated.at[me], s_d.at[q], r_d.at[q], sp=dest(2 * q))

    def gated_over(q):
        piece = gated.at[source(2 * q)]
        return remote(piece, piece, s_p.at[q], r_p.at[q], sp=dest(1))

    for load in early[:2]:
        load.wait()
    names = lax.broadcasted_iota(jnp.int32, (n, tokens), 0)
    chosen = jnp.zeros((n, tokens), jnp.bool_)
    weights = jnp.zeros((n, tokens), F32)
    for choice in range(routes.shape[0]):
        named = names == routes[choice : choice + 1, :]
        chosen = jnp.logical_or(chosen, named)
        weights = weights + jnp.where(named, route_weight[choice : choice + 1, :], 0.0)
    first = lax.broadcasted_iota(jnp.int32, (tokens, tokens), 0)
    second = lax.broadcasted_iota(jnp.int32, (tokens, tokens), 1)
    earlier = jnp.where(first < second, 1.0, 0.0).astype(BF16)
    marks = jnp.where(chosen, 1.0, 0.0)
    places = jnp.where(chosen, dot_nn(marks.astype(BF16), earlier), -1.0)
    for e in range(n):
        place[e] = places[e : e + 1, :]
        weight[e] = weights[e : e + 1, :]
    seats = lax.broadcasted_iota(jnp.int32, (slots, tokens), 0).astype(F32)

    def pick(e):
        filled = place[e] == seats
        found = jnp.where(filled, 1.0, 0.0).astype(BF16)
        picker[e] = found
        held = jnp.sum(jnp.where(filled, weight[e], 0.0), axis=1, keepdims=True)
        return found, held

    for load in early[2:]:
        load.wait()
    pl.semaphore_wait(barrier, n + 1)
    for i, ref in enumerate((in_gate, conv_input)):
        rim_copy(i, ref).start()

    def build(k, carry):
        e = dest(k)
        found, held = pick(e)
        own = dot_nn(found, out_grad[:, columns(member, share)])
        send[e] = (held * own).astype(BF16)
        across(k).start()
        return carry

    lax.fori_loop(1, n, build, 0)
    found, held = pick(me)
    for g in range(groups):
        at = pl.ds(g * share, share)
        grads[me, :, at] = (held * dot_nn(found, out_grad[:, at])).astype(BF16)
    for load in loads[:3]:
        load.wait()
    couples = 2

    def project(c, carry):
        at = pl.ds(c * couples, couples)
        rows_c = rows[at].reshape(couples * slots, width)
        hidden[at] = dot_nn(rows_c, wgu[...]).reshape(couples, slots, 2 * ff)
        return carry

    lax.fori_loop(0, n // couples, project, 0)

    for i, ref in enumerate((in_gate, conv_input)):
        rim_copy(i, ref).wait_recv()
    prior = rim[0].astype(F32) * rim[1].astype(F32)
    mixed[0:16] = jnp.where(me == 0, 0.0, prior)
    mixed[pl.ds(16, tokens)] = in_gate[...].astype(F32) * conv_input[...].astype(F32)
    reach = taps.shape[0]
    conv_sum = taps[0:1, :] * mixed[pl.ds(16, tokens)]
    for tap in range(1, reach):
        conv_sum = conv_sum + taps[tap : tap + 1, :] * mixed[pl.ds(16 - tap, tokens)]
    conv[...] = conv_sum
    gated[me] = (out_gate[...].astype(F32) * conv_sum).astype(BF16)
    for q in range(1, deep):
        gated_along(q).start()
    gated_over(0).start()
    loads[3].wait()
    loads[4].wait()

    def arrive(k):
        across(k).wait_recv()
        cross(k).start()
        hand(k).start()

    def pass_on(k):
        cross(k).wait_recv()
        relay(k).start()

    def backward(k):
        @pl.when(k > 0)
        def _():
            hand(k).wait_recv()
            relay(k).wait_recv()

        s = source(k)
        gate = hidden[s, :, 0:ff]
        up = hidden[s, :, ff : 2 * ff]
        sig = jax.nn.sigmoid(gate)
        act[s] = (gate * sig * up).astype(BF16)
        act_grad = dot_nt(grads[s], dn[...])
        parts[s, :, 0:ff] = (act_grad * up * sig * (1.0 + gate * (1.0 - sig))).astype(BF16)
        parts[s, :, ff : 2 * ff] = (act_grad * gate * sig).astype(BF16)
        both = parts[s]
        for g in range(groups):
            at = pl.ds(g * share, share)
            row_part[s, :, at] = dot_nt(both, wgu[at, :]).astype(BF16)
        for h in range(2):
            to_sibling(k, h).start()

    def pair_up(k):
        s = source(k)
        for h in range(2):
            to_sibling(k, h).wait_recv()
            mine = row_part[s, :, columns(2 * h + seat, share)].astype(F32)
            pair[s, h] = (mine + near[s, h].astype(F32)).astype(BF16)
        to_other(k).start()

    def finish(k):
        s = source(k)
        to_other(k).wait_recv()
        final[s] = (pair[s, line].astype(F32) + far[s].astype(F32)).astype(BF16)

        @pl.when(k > 0)
        def _():
            to_home(k).start()

    def within(k, low, act_on):
        @pl.when(jnp.logical_and(k >= low, k < n))
        def _():
            act_on(k)

    def step(j, carry):
        within(j + 1, 1, arrive)
        within(j, 1, pass_on)
        within(j - 1, 0, backward)
        within(j - 2, 0, pair_up)
        within(j - 3, 0, finish)
        return carry

    lax.fori_loop(0, n + 3, step, 0)

    for q in range(1, deep):
        gated_along(q).wait_recv()
        gated_over(q).start()

    total[...] = out_grad[:, columns(member, share)].astype(F32) + dot_tn(picker[me], final[me])

    def gather_home(k, carry):
        e = dest(k)
        to_home(k).wait_recv()
        total[...] += dot_tn(picker[e], back[e])
        return carry

    lax.fori_loop(1, n, gather_home, 0)
    mid = total[...].astype(BF16)
    mid_out[...] = mid
    wide[:, columns(member, share)] = mid

    def mid_sibling():
        piece = wide.at[:, columns(member, share)]
        return remote(piece, piece, s_m, r_m, tp=sibling)

    def mid_other(q):
        piece = wide.at[:, slice_at(member * per + q)]
        return remote(piece, piece, s_mx.at[q], r_mx.at[q], tp=other)

    def mid_relay(q):
        piece = wide.at[:, slice_at(other * per + q)]
        return remote(piece, piece, s_mr.at[q], r_mr.at[q], tp=sibling)

    def slice_out(j):
        return remote(wide.at[:, slice_at(j)], slices.at[me], s_v.at[j], r_v.at[me], sp=j)

    def slice_in(s):
        return remote(wide.at[:, slice_at(me)], slices.at[s], s_v.at[s], r_v.at[s], sp=s)

    def slice_relay(s):
        piece = slices.at[s]
        return remote(piece, piece, s_w.at[s], r_w.at[s], tp=sibling)

    def send_slice(j):
        @pl.when(j != me)
        def _():
            slice_out(j).start()

    for q in range(per):
        mid_other(q).start()
    mid_sibling().start()
    for q in range(per):
        send_slice(member * per + q)

    chunk = 128 if width % 256 else 256
    chunks = width // chunk

    def weigh(piece, carry):
        at = columns(piece, chunk)
        tall = n * slots
        grown = dot_tn(rows[:, :, at].reshape(tall, chunk), parts[...].reshape(tall, 2 * ff))
        gate_out[at, :] = grown[:, 0:ff].astype(BF16)
        up_out[at, :] = grown[:, ff : 2 * ff].astype(BF16)
        down_out[:, at] = dot_tn(
            act[...].reshape(tall, ff), grads[:, :, at].reshape(tall, chunk)
        ).astype(BF16)
        return carry

    lax.fori_loop(0, chunks // 2, weigh, 0)
    for q in range(per):
        mid_other(q).wait_recv()
        mid_relay(q).start()
        send_slice(other * per + q)
    lax.fori_loop(chunks // 2, chunks, weigh, 0)
    mid_sibling().wait_recv()
    for q in range(per):
        mid_relay(q).wait_recv()
    gated_grad = dot_nn(wide[...], ow[...])
    conv_grad = gated_grad * out_gate[...].astype(F32)
    follow[pl.ds(0, tokens)] = conv_grad

    back_rim = remote(
        follow.at[pl.ds(0, 8)], later, s_l, r_l, sp=lax.rem(me + n - 1, n)
    )
    back_rim.start()
    out_gate_out[...] = (gated_grad * conv[...]).astype(BF16)
    for q in range(deep):
        gated_over(q).wait_recv()
    holder = lax.rem(lax.div(me, per), 2)

    def meet(off, carry):
        s = lax.rem(me + off, n)

        @pl.when(holder == seat)
        def _():
            slice_in(s).wait_recv()
            slice_relay(s).start()

        @pl.when(holder != seat)
        def _():
            slice_relay(s).wait_recv()

        return carry

    lax.fori_loop(1, n, meet, 0)
    slices[me] = wide[:, slice_at(me)]
    weight_out[...] = dot_tn(
        slices[...].reshape(n * tokens, span), gated[...].reshape(n * tokens, gated.shape[2])
    )
    back_rim.wait_recv()
    follow[pl.ds(tokens, 8)] = jnp.where(me == n - 1, 0.0, later[...])
    mixed_grad = taps[0:1, :] * follow[pl.ds(0, tokens)]
    for tap in range(1, reach):
        mixed_grad = mixed_grad + taps[tap : tap + 1, :] * follow[pl.ds(tap, tokens)]
    input_out[...] = (mixed_grad * in_gate[...].astype(F32)).astype(BF16)
    in_gate_out[...] = (mixed_grad * conv_input[...].astype(F32)).astype(BF16)

    def drain(k, carry):
        @pl.when(k > 0)
        def _():
            across(k).wait_send()
            hand(k).wait_send()
            cross(k).wait_send()
            relay(k).wait_send()
            to_home(k).wait_send()

        for h in range(2):
            to_sibling(k, h).wait_send()
        to_other(k).wait_send()
        return carry

    lax.fori_loop(0, n, drain, 0)

    def drain_slices(off, carry):
        s = lax.rem(me + off, n)

        @pl.when(holder == seat)
        def _():
            slice_relay(s).wait_send()

        return carry

    lax.fori_loop(1, n, drain_slices, 0)
    for i, ref in enumerate((in_gate, conv_input)):
        rim_copy(i, ref).wait_send()
    for q in range(deep):
        gated_over(q).wait_send()
        if q > 0:
            gated_along(q).wait_send()
    mid_sibling().wait_send()
    back_rim.wait_send()
    for q in range(per):
        mid_other(q).wait_send()
        mid_relay(q).wait_send()
        for owner in (member, other):

            @pl.when(owner * per + q != me)
            def _():
                slice_out(owner * per + q).wait_send()


def settle_kernel(count, *refs):
    sources, targets, sem = refs[:count], refs[count : 2 * count], refs[2 * count]
    moves = [pltpu.make_async_copy(a, b, sem.at[i]) for i, (a, b) in enumerate(zip(sources, targets))]
    for move in moves:
        move.start()
    for move in moves:
        move.wait()


def settle(arrays):
    count = len(arrays)
    return pl.pallas_call(
        functools.partial(settle_kernel, count),
        out_shape=tuple(jax.ShapeDtypeStruct(a.shape, a.dtype) for a in arrays),
        in_specs=[ANY_SPEC] * count,
        out_specs=(HBM_SPEC,) * count,
        scratch_shapes=[pltpu.SemaphoreType.DMA((count,))],
        compiler_params=pltpu.CompilerParams(vmem_limit_bytes=2**20),
    )(*arrays)


def fused(
    out_grad,
    routes,
    route_weight,
    rows,
    gate_weight,
    up_weight,
    down_weight,
    conv_input,
    out_gate,
    in_gate,
    taps,
    out_weight,
    groups,
):
    n, slots, width = rows.shape
    tokens = out_grad.shape[0]
    ff = gate_weight.shape[1]
    chans = conv_input.shape[1]
    share, span, deep, per = width // groups, width // n, n // 2, n // groups
    dma = pltpu.SemaphoreType.DMA

    def held(*shape):
        return pltpu.VMEM(shape, BF16)

    def exact(*shape):
        return pltpu.VMEM(shape, F32)

    operands = (
        out_grad,
        routes.T,
        route_weight.T,
        conv_input,
        out_gate,
        in_gate,
        taps,
        rows,
        gate_weight,
        up_weight,
        down_weight,
        out_weight,
    )
    small = held(tokens, chans)
    return pl.pallas_call(
        functools.partial(fused_kernel, n, groups),
        out_shape=(
            held(width, ff),
            held(width, ff),
            held(ff, width),
            held(tokens, share),
            exact(span, chans),
            small,
            small,
            small,
        ),
        in_specs=[HBM_SPEC] * 12,
        out_specs=(VMEM_SPEC,) * 8,
        scratch_shapes=[
            held(tokens, width),
            pltpu.VMEM(routes.T.shape, routes.dtype),
            exact(*route_weight.T.shape),
            held(tokens, chans),
            held(tokens, chans),
            held(tokens, chans),
            exact(*taps.shape),
            held(n, slots, width),
            held(width, 2 * ff),
            held(ff, width),
            held(width, chans),
            exact(n, slots, 2 * ff),
            exact(n, 1, tokens),
            exact(n, 1, tokens),
            held(n, slots, tokens),
            held(n, slots, share),
            held(n, slots, width),
            held(n, slots, ff),
            held(n, slots, 2 * ff),
            held(n, slots, width),
            held(n, 2, slots, share),
            held(n, 2, slots, share),
            held(n, slots, share),
            held(n, slots, share),
            held(n, slots, share),
            exact(tokens, share),
            held(tokens, width),
            held(2, 16, chans),
            exact(16 + tokens, chans),
            exact(tokens, chans),
            held(n, tokens, chans),
            held(n, tokens, span),
            exact(tokens + 8, chans),
            exact(8, chans),
            dma((12,)),
        ]
        + [dma((n,))] * 8
        + [dma((2, n))] * 2
        + [dma((n,))] * 4
        + [dma((2,))] * 2
        + [dma((deep,))] * 4
        + [dma(())] * 2
        + [dma((per,))] * 4
        + [dma((n,))] * 4
        + [dma(())] * 2,
        compiler_params=pltpu.CompilerParams(
            collective_id=4, has_side_effects=True, vmem_limit_bytes=40 * 2**20
        ),
    )(*(pltpu.with_memory_space_constraint(a, pltpu.HBM) for a in operands))


def fits_fused(tokens, slots, width, sources, groups):
    tidy = slots % 16 == 0 and tokens % 16 == 0 and width % (128 * sources) == 0
    return tidy and groups == 4 and sources % 4 == 0


def on_device(
    out_grad,
    routes,
    route_weight,
    expert_rows,
    gate_weight,
    up_weight,
    down_weight,
    conv_input,
    out_gate,
    in_gate,
    taps,
    out_weight,
):
    groups = lax.axis_size("tp")
    sources = lax.axis_size("sp")
    slots, width = expert_rows.shape[2:]
    assert gate_weight.shape[0] == 1
    if not fits_fused(out_grad.shape[0], slots, width, sources, groups):
        return staged(
            out_grad,
            routes,
            route_weight,
            expert_rows,
            gate_weight,
            up_weight,
            down_weight,
            conv_input,
            out_gate,
            in_gate,
            taps,
            out_weight,
        )
    outs = fused(
        out_grad,
        routes,
        route_weight,
        expert_rows.reshape(sources, slots, width),
        gate_weight[0],
        up_weight[0],
        down_weight[0],
        conv_input,
        out_gate,
        in_gate,
        taps,
        out_weight,
        groups,
    )
    outs = settle(outs)
    return tuple(out[None] for out in outs[:3]) + tuple(outs[3:])


def staged(
    out_grad,
    routes,
    route_weight,
    expert_rows,
    gate_weight,
    up_weight,
    down_weight,
    conv_input,
    out_gate,
    in_gate,
    taps,
    out_weight,
):
    groups = lax.axis_size("tp")
    member = lax.axis_index("tp")
    sources = lax.axis_size("sp")
    tok_rows, width = out_grad.shape
    top = routes.shape[1]
    local = gate_weight.shape[0]
    assert local == 1
    experts = local * sources
    slots = expert_rows.shape[2]
    share = width // groups
    own_cols = lax.dynamic_slice_in_dim(out_grad, member * share, share, 1)
    names = jnp.arange(experts, dtype=jnp.int32)
    named = routes[:, :, None] == names[None, None, :]
    chosen = jnp.any(named, axis=1)
    weight = jnp.sum(jnp.where(named, route_weight[:, :, None], 0.0), axis=1)
    order = jnp.arange(tok_rows, dtype=jnp.int32)
    earlier = (order[:, None] > order[None, :]).astype(jnp.bfloat16)
    place = jnp.dot(
        earlier, chosen.astype(jnp.bfloat16), preferred_element_type=jnp.float32
    ).astype(jnp.int32)
    place = jnp.where(chosen, place, -1).T
    filled = place[:, None, :] == jnp.arange(slots, dtype=jnp.int32)[None, :, None]
    slot_weight = jnp.sum(jnp.where(filled, weight.T[:, None, :], 0.0), axis=2)
    picker = filled.astype(jnp.bfloat16).reshape(experts * slots, tok_rows)
    outgoing = jnp.dot(picker, own_cols, preferred_element_type=jnp.float32)
    outgoing = (slot_weight.reshape(-1, 1) * outgoing).astype(jnp.bfloat16)
    outgoing = outgoing.reshape(sources, local * slots, share)
    rows = expert_rows.reshape(-1, width)
    wide_gate, wide_up, tall_down = gate_weight[0], up_weight[0], down_weight[0]
    grads, gate, up = spread(outgoing, rows, wide_gate, wide_up, groups)
    grads = grads.reshape(-1, width)
    sig = jax.nn.sigmoid(gate)
    act = (gate * sig * up).astype(jnp.bfloat16)
    act_grad = lax.dot_general(
        grads, tall_down, (((1,), (1,)), ((), ())), preferred_element_type=jnp.float32
    )
    up_part = (act_grad * gate * sig).astype(jnp.bfloat16)
    gate_part = (act_grad * up * sig * (1.0 + gate * (1.0 - sig))).astype(jnp.bfloat16)
    row_part = lax.dot_general(
        gate_part, wide_gate, (((1,), (1,)), ((), ())), preferred_element_type=jnp.float32
    )
    row_part = row_part + lax.dot_general(
        up_part, wide_up, (((1,), (1,)), ((), ())), preferred_element_type=jnp.float32
    )
    row_part = row_part.astype(jnp.bfloat16).reshape(sources, slots, width)
    returned, gate_grad, up_grad, down_grad = collect(
        row_part, rows, grads, act, gate_part, up_part, groups
    )
    returned = returned.reshape(experts * slots, share)
    gate_grad, up_grad, down_grad = gate_grad[None], up_grad[None], down_grad[None]
    picked = lax.dot_general(
        picker, returned, (((0,), (0,)), ((), ())), preferred_element_type=jnp.float32
    )
    mid_grad = (own_cols.astype(jnp.float32) + picked).astype(jnp.bfloat16)
    mid_whole = widen(mid_grad, groups)
    reach = taps.shape[0] - 1
    rims = jnp.stack([in_gate[tok_rows - reach :], conv_input[tok_rows - reach :]])
    prior = passed_along(rims, "sp", 1)
    mixed = in_gate.astype(jnp.float32) * conv_input.astype(jnp.float32)
    prior_mixed = prior[0].astype(jnp.float32) * prior[1].astype(jnp.float32)
    extended = jnp.concatenate([prior_mixed, mixed], axis=0)
    conv = jnp.zeros_like(mixed)
    for tap in range(reach + 1):
        conv = conv + taps[tap][None, :] * extended[reach - tap : reach - tap + tok_rows]
    gated = (out_gate.astype(jnp.float32) * conv).astype(jnp.bfloat16)
    partial_grad = lax.dot_general(
        mid_whole, gated, (((0,), (0,)), ((), ())), preferred_element_type=jnp.float32
    ).astype(jnp.bfloat16)
    out_weight_grad = fold(partial_grad.reshape(sources, width // sources, gated.shape[1]))
    gated_grad = jnp.dot(mid_whole, out_weight, preferred_element_type=jnp.float32)
    out_gate_grad = (gated_grad * conv).astype(jnp.bfloat16)
    conv_grad = gated_grad * out_gate.astype(jnp.float32)
    later = passed_along(conv_grad[:reach], "sp", -1)
    following = jnp.concatenate([conv_grad, later], axis=0)
    mixed_grad = jnp.zeros_like(conv_grad)
    for tap in range(reach + 1):
        mixed_grad = mixed_grad + taps[tap][None, :] * following[tap : tap + tok_rows]
    input_grad = (mixed_grad * in_gate.astype(jnp.float32)).astype(jnp.bfloat16)
    in_gate_grad = (mixed_grad * conv_input.astype(jnp.float32)).astype(jnp.bfloat16)
    return (
        gate_grad,
        up_grad,
        down_grad,
        mid_grad,
        out_weight_grad,
        input_grad,
        out_gate_grad,
        in_gate_grad,
    )


def solution(mesh):
    in_specs = (
        P("sp", None),
        P("sp", None),
        P("sp", None),
        P(None, "sp", None, None),
        P("sp", None, "tp"),
        P("sp", None, "tp"),
        P("sp", "tp", None),
        P("sp", "tp"),
        P("sp", "tp"),
        P("sp", "tp"),
        P(None, "tp"),
        P(None, "tp"),
    )
    out_specs = (
        P("sp", None, "tp"),
        P("sp", None, "tp"),
        P("sp", "tp", None),
        P("sp", "tp"),
        P("sp", "tp"),
        P("sp", "tp"),
        P("sp", "tp"),
        P("sp", "tp"),
    )
    return jax.shard_map(
        on_device, mesh=mesh, in_specs=in_specs, out_specs=out_specs, check_vma=False
    )
```
